256 devices in a mesh: sp: 64 (over z, y, core), tp: 4 (over x).
Axes of the slice: x: 4, y: 4, z: 8, core: 2. Of those that a mesh axis runs over, the one named last changes fastest.
Arguments:
- block_input: bfloat16 [65536, 2048], P('sp'), may hold values from -6 to 6
- out_grad: bfloat16 [65536, 2048], P('sp'), may hold values from -16 to 16
- w_value: bfloat16 [2048, 1024], P(None, 'tp'), may hold values from -0.125 to 0.125
- w_gate: bfloat16 [2048, 1024], P(None, 'tp'), may hold values from -0.125 to 0.125
- conv_taps: float32 [31, 1024], P(None, 'tp'), may hold values from -4 to 4
- norm_gain: float32 [1024], P('tp'), may hold values from 0.1 to 1.9
- norm_shift: float32 [1024], P('tp'), may hold values from -3 to 3
- w_proj: bfloat16 [1024, 2048], P('tp'), may hold values from -0.1875 to 0.1875
Outputs:
- input_grad: bfloat16 [65536, 2048], P('sp', 'tp')
- value_wgrad: float32 [2048, 1024], P('sp', 'tp')
- gate_wgrad: float32 [2048, 1024], P('sp', 'tp')
- proj_wgrad: float32 [1024, 2048], P('tp', 'sp')
- taps_grad: float32 [31, 1024], P(None, 'tp')
- gain_grad: float32 [1024], P('tp')
- shift_grad: float32 [1024], P('tp')
The draws below stay inside these ranges and needn't reach their ends.
All inputs are finite; a program needn't handle non-finite values.
Results may differ from the reference program's by a relative error of at most 0.014.
Values may be sent and summed in bfloat16 or wider, within the bound.
A program may use at most 128 MiB of HBM per device.

```python
import math
import jax
import jax.numpy as jnp
from jax import lax

D = 2048
CH = 1024
KERNEL = 31
TOKENS = 65536
N_TP = 4


def draw_conv_taps(key, part):
    base = jax.random.fold_in(key, 11)
    first, second, third = jax.random.split(base, 3)
    channel = jnp.arange(CH, dtype=jnp.float32)
    phase = jax.random.uniform(first, (), jnp.float32, 0.0, 6.2831)
    level = jnp.exp(1.2 * jnp.sin(6.2831853 * channel / CH + phase))
    rough = jnp.exp(jax.random.uniform(second, (CH,), jnp.float32, -0.7, 0.7))
    taps = jax.random.truncated_normal(third, -3.0, 3.0, (KERNEL, CH), jnp.float32)
    return (taps * (level * rough)[None, :] / math.sqrt(KERNEL)).astype(jnp.float32)


def with_spikes(entries, rng, source, target, parts, factor):
    def block_of(dim):
        return (jnp.arange(entries.shape[dim]) // (entries.shape[dim] // parts)).reshape((-1,) + (1,) * (entries.ndim - 1 - dim))

    one_side = jax.random.permutation(rng, parts)[block_of(target)]
    other_side = (block_of(target) + parts // 2) % parts
    return jnp.where((block_of(source) == one_side) | (block_of(source) == other_side), factor * entries, entries)


def shard_levels(rng, dims, cuts, low, top_value):
    def one(dim, shards_of):
        steps = jax.random.uniform(jax.random.fold_in(jax.random.fold_in(rng, 6), dim), (shards_of,), jnp.float32, low / len(cuts), top_value / len(cuts))
        return jnp.repeat(jnp.exp(steps), dims[dim] // shards_of).reshape((-1,) + (1,) * (len(dims) - dim - 1))

    gain = one(*cuts[0])
    for cut in cuts[1:]:
        gain = gain * one(*cut)
    return gain


def scatter_about(stream_key, dims, spread, reach, pieces=(), kind=jnp.bfloat16):
    result = spread * jax.random.normal(stream_key, dims, jnp.float32)
    if pieces:
        result = result * shard_levels(stream_key, dims, pieces, -0.22, 0.18)
    return jnp.clip(result, -reach, reach).astype(kind)


def gaussian_with(own_key, dims, scale, limit, cuts, heavy, kind=jnp.bfloat16):
    entries = scale * jax.random.normal(own_key, dims, jnp.float32)
    if cuts:
        entries = entries * shard_levels(own_key, dims, cuts, -0.22, 0.18)
    return jnp.clip(with_spikes(entries, jax.random.fold_in(own_key, 3), *heavy), -limit, limit).astype(kind)


def setup_inputs(seed: int = 0) -> dict:
    streams_of = jax.random.split(jax.random.key(seed), 9)
    block_input = scatter_about(streams_of[0], (TOKENS, D), 1.0, 6.0, ((0, 64),))
    out_grad = gaussian_with(streams_of[1], (TOKENS, D), 1.0, 16.0, ((0, 64),), (0, 1, 64, 4.0))
    w_value = scatter_about(streams_of[2], (D, CH), D ** -0.5, 0.125, ((1, 4),))
    w_gate = scatter_about(streams_of[3], (D, CH), D ** -0.5, 0.125, ((1, 4),))
    conv_taps = draw_conv_taps(jax.random.fold_in(streams_of[8], 71), 0)
    norm_gain = jnp.clip(1.0 + 0.18 * jax.random.normal(streams_of[5], (CH,), jnp.float32), 0.1, 1.9)
    norm_shift = scatter_about(streams_of[6], (CH,), 0.5, 3.0, ((0, 4),), jnp.float32)
    w_proj = scatter_about(streams_of[7], (CH, D), CH ** -0.5, 0.1875, ((0, 4),))
    return {"block_input": block_input, "out_grad": out_grad, "w_value": w_value, "w_gate": w_gate, "conv_taps": conv_taps, "norm_gain": norm_gain, "norm_shift": norm_shift, "w_proj": w_proj}


EPS = 0.05

def reference(block_input, out_grad, w_value, w_gate, conv_taps, norm_gain, norm_shift, w_proj):
    value_proj = jnp.dot(block_input, w_value, preferred_element_type=jnp.float32).astype(jnp.bfloat16)
    gate_proj = jnp.dot(block_input, w_gate, preferred_element_type=jnp.float32).astype(jnp.bfloat16)
    gate_sigmoid = jax.nn.sigmoid(gate_proj.astype(jnp.float32))
    value_wide = value_proj.astype(jnp.float32)
    gated_input = (value_wide * gate_sigmoid).astype(jnp.bfloat16)
    padded_glu = jnp.pad(gated_input.astype(jnp.float32), ((KERNEL - 1, 0), (0, 0)))
    filtered = jnp.zeros((TOKENS, CH), jnp.float32)
    for tap_index in range(KERNEL):
        begin = KERNEL - 1 - tap_index
        filtered = filtered + conv_taps[tap_index] * padded_glu[begin:begin + TOKENS]
    row_mean = lax.optimization_barrier(jnp.sum(filtered, axis=1)) / CH
    row_var = lax.optimization_barrier(jnp.sum(filtered * filtered, axis=1)) / CH - row_mean * row_mean
    row_scale = lax.rsqrt(row_var + EPS)
    normed = (filtered - row_mean[:, None]) * row_scale[:, None]
    activated = normed * norm_gain + norm_shift
    act_sigmoid = jax.nn.sigmoid(activated)
    mixer_out = (activated * act_sigmoid).astype(jnp.bfloat16)
    grad_mixed = jnp.dot(out_grad, w_proj.T, preferred_element_type=jnp.float32)
    grad_act = grad_mixed * act_sigmoid * (1.0 + activated * (1.0 - act_sigmoid))
    grad_normed = grad_act * norm_gain
    first_mean = lax.optimization_barrier(jnp.sum(grad_normed, axis=1)) / CH
    second_mean = lax.optimization_barrier(jnp.sum(grad_normed * normed, axis=1)) / CH
    grad_filtered = row_scale[:, None] * (grad_normed - first_mean[:, None] - normed * second_mean[:, None])
    padded_grad = jnp.pad(grad_filtered, ((0, KERNEL - 1), (0, 0)))
    grad_glu = jnp.zeros((TOKENS, CH), jnp.float32)
    taps_rows = []
    for tap_index in range(KERNEL):
        begin = KERNEL - 1 - tap_index
        grad_glu = grad_glu + conv_taps[tap_index] * padded_grad[tap_index:tap_index + TOKENS]
        taps_rows.append(lax.optimization_barrier(jnp.sum(grad_filtered * padded_glu[begin:begin + TOKENS], axis=0)))
    grad_value = (grad_glu * gate_sigmoid).astype(jnp.bfloat16)
    grad_gate = (grad_glu * value_wide * gate_sigmoid * (1.0 - gate_sigmoid)).astype(jnp.bfloat16)
    block_cols = CH // N_TP
    summed = jnp.zeros((TOKENS, D), jnp.float32)
    for block_index in range(N_TP):
        low = block_index * block_cols
        high = low + block_cols
        partial_sum = jnp.dot(grad_value[:, low:high], w_value[:, low:high].T, preferred_element_type=jnp.float32)
        partial_sum = partial_sum + jnp.dot(grad_gate[:, low:high], w_gate[:, low:high].T, preferred_element_type=jnp.float32)
        summed = summed + partial_sum.astype(jnp.bfloat16).astype(jnp.float32)
    input_grad = summed.astype(jnp.bfloat16)
    loss_scale = 1.0 / jnp.sqrt(jnp.float32(TOKENS))
    value_wgrad = jnp.dot(block_input.T, grad_value, preferred_element_type=jnp.float32) * loss_scale
    gate_wgrad = jnp.dot(block_input.T, grad_gate, preferred_element_type=jnp.float32) * loss_scale
    proj_wgrad = jnp.dot(mixer_out.T, out_grad, preferred_element_type=jnp.float32) * loss_scale
    taps_grad = jnp.stack(taps_rows, axis=0) * loss_scale
    gain_grad = lax.optimization_barrier(jnp.sum(grad_act * normed, axis=0)) * loss_scale
    shift_grad = lax.optimization_barrier(jnp.sum(grad_act, axis=0)) * loss_scale
    return (input_grad, value_wgrad, gate_wgrad, proj_wgrad, taps_grad, gain_grad, shift_grad)
```

```python
import functools
import math

import jax
import jax.numpy as jnp
from jax import lax
from jax.experimental import pallas as pl
from jax.experimental.pallas import tpu as pltpu
from jax.sharding import PartitionSpec as P

CH = 1024
SP = "sp"
MESH = pl.DeviceIdType.MESH
BF = jnp.bfloat16
F32 = jnp.float32


EPS = 0.05


def from_behind(block, axis, distance):
    devices = range(lax.axis_size(axis))
    route = [(i - distance, i) for i in devices if i - distance in devices]
    return lax.ppermute(block, axis, route)


def sent_to_all(x, axis):
    length = lax.axis_size(axis)
    return lax.all_to_all(jnp.broadcast_to(x[None], (length, *x.shape)), axis, 0, 0, tiled=True)


def of_everyone(x, axis):
    return sent_to_all(x, axis).sum(axis=0)


def together(arrays, axis):
    ravelled, at, gathered = (jnp.concatenate([a.reshape(-1) for a in arrays]), 0, [])
    subtotal = of_everyone(ravelled, axis)
    for a in arrays:
        gathered.append(subtotal[at : at + a.size].reshape(a.shape))
        at += a.size
    return tuple(gathered)


def right_product(left, right):
    return lax.dot_general(
        left, right, (((1,), (1,)), ((), ())), preferred_element_type=jnp.float32
    )


def column_product(left, right):
    return lax.dot_general(
        left, right, (((0,), (0,)), ((), ())), preferred_element_type=jnp.float32
    )


def rows_product(left, right):
    return lax.dot_general(left, right, (((1,), (1,)), ((), ())), preferred_element_type=F32)


def cols_product(left, right):
    return lax.dot_general(left, right, (((0,), (0,)), ((), ())), preferred_element_type=F32)


def back_kernel(
    scale,
    x, g, gb, mx, wv, wg, sm,
    ig_out, v_out, g_out, p_out, sm_out,
    part, own, got_a, got_b, got_c,
    wbuf, got_w, s1, got_y, s2, got_z,
    smb, sm_c, sm_y, sm_z,
    xs, xr, cs, cr, ys, yr, zs, zr, ms, mr,
):
    s = lax.axis_index(SP)
    t = lax.axis_index("tp")
    c, y, z = s % 2, (s // 2) % 4, s // 8
    right, left, far = (t + 1) % 4, (t + 3) % 4, (t + 2) % 4
    half, cols = part.shape[2], part.shape[3]

    def at_y(k):
        return {SP: (z * 4 + (y + k) % 4) * 2 + c}

    def at_z(k):
        return {SP: (((z + k) % 8) * 4 + y) * 2 + c}

    partner = {SP: s + 1 - 2 * c}
    peers = [{"tp": (t + k) % 4} for k in (1, 2, 3)] + [partner]
    peers += [at_y(k) for k in (1, 2, 3)] + [at_z(k) for k in range(1, 8)]
    barrier = pltpu.get_barrier_semaphore()
    for peer in peers:
        pl.semaphore_signal(barrier, inc=1, device_id=peer, device_id_type=MESH)
    pl.semaphore_wait(barrier, len(peers))

    def send(src, dst, ssem, rsem, device):
        copy = pltpu.make_async_remote_copy(
            src_ref=src, dst_ref=dst, send_sem=ssem, recv_sem=rsem,
            device_id=device, device_id_type=MESH,
        )
        copy.start()
        return copy

    sm_copy = send(sm, sm_c, ms.at[0], mr.at[0], partner)

    def partial(block, h):
        rows = pl.ds(h * half, half)
        span = pl.ds(pl.multiple_of(block * cols, cols), cols)
        return rows_product(gb[rows, 0:256], wv[span, :]) + rows_product(
            gb[rows, 256:512], wg[span, :]
        )

    to_right, to_left = {"tp": right}, {"tp": left}
    part[0, 0] = partial(far, 0).astype(BF)
    a_r = send(part.at[0, 0], got_a.at[0], xs.at[0], xr.at[0], to_right)
    part[0, 1] = partial(far, 1).astype(BF)
    a_l = send(part.at[0, 1], got_a.at[1], xs.at[1], xr.at[1], to_left)
    part[1, 1] = partial(right, 1).astype(BF)
    b_r = send(part.at[1, 1], got_b.at[0], xs.at[2], xr.at[2], to_right)
    part[2, 0] = partial(left, 0).astype(BF)
    b_l = send(part.at[2, 0], got_b.at[1], xs.at[3], xr.at[3], to_left)

    sm_copy.wait_recv()
    smb[0] = sm[...] + sm_c[...]
    sm_ys = [send(smb.at[0], sm_y.at[k - 1], ms.at[k], mr.at[k], at_y(k)) for k in (1, 2, 3)]

    w_copies = []
    for n in range(3):
        source, right_side, off = (g, mx, 0) if n == 0 else (x, gb, (n - 1) * 256)

        def weight_tile(zb, _, n=n, source=source, right_side=right_side, off=off):
            span = pl.ds(pl.multiple_of(zb * 256, 256), 256)
            tile = cols_product(source[:, span], right_side[:, off : off + 256])
            wbuf[n, pl.ds(zb * 4, 4)] = tile.astype(BF).reshape(4, 2, 32, 256)
            return 0

        lax.fori_loop(0, 8, weight_tile, 0)
        w_copies.append(
            send(wbuf.at[n, :, 1 - c], got_w.at[n], cs.at[n], cr.at[n], partner)
        )

    y_copies = []
    for n in range(3):
        w_copies[n].wait_recv()

        def pair_sum(zb, _, n=n):
            rows = pl.ds(zb * 4, 4)
            pair = wbuf[n, rows, c].astype(F32) + got_w[n, rows].astype(F32)
            s1[n, zb] = pair.astype(BF)
            return 0

        lax.fori_loop(0, 8, pair_sum, 0)
        y_copies.append(
            [
                send(s1.at[n, :, (y + k) % 4], got_y.at[n, k - 1], ys.at[n, k - 1],
                     yr.at[n, k - 1], at_y(k))
                for k in (1, 2, 3)
            ]
        )

    part[1, 0] = partial(right, 0).astype(BF)
    part[2, 1] = partial(left, 1).astype(BF)
    own[0] = partial(t, 0)
    own[1] = partial(t, 1)

    for copy in sm_ys:
        copy.wait_recv()
    smb[1] = smb[0] + sm_y[0] + sm_y[1] + sm_y[2]
    sm_zs = [
        send(smb.at[1], sm_z.at[k - 1], ms.at[3 + k], mr.at[3 + k], at_z(k)) for k in range(1, 8)
    ]

    a_r.wait_recv()
    part[1, 0] = (part[1, 0].astype(F32) + got_a[0].astype(F32)).astype(BF)
    c_r = send(part.at[1, 0], got_c.at[0], xs.at[4], xr.at[4], to_right)
    a_l.wait_recv()
    part[2, 1] = (part[2, 1].astype(F32) + got_a[1].astype(F32)).astype(BF)
    c_l = send(part.at[2, 1], got_c.at[1], xs.at[5], xr.at[5], to_left)

    z_copies = []
    for n in range(3):
        for copy in y_copies[n]:
            copy.wait_recv()
        total = s1[n, :, y].astype(F32)
        for k in range(3):
            total = total + got_y[n, k].astype(F32)
        s2[n] = total.astype(BF)
        z_copies.append(
            [
                send(s2.at[n, (z + k) % 8], got_z.at[n, k - 1], zs.at[n, k - 1],
                     zr.at[n, k - 1], at_z(k))
                for k in range(1, 8)
            ]
        )

    for copy in sm_zs:
        copy.wait_recv()
    total = smb[1]
    for k in range(7):
        total = total + sm_z[k]
    sm_out[...] = total * scale

    for n, out in enumerate((p_out, v_out, g_out)):
        for copy in z_copies[n]:
            copy.wait_recv()
        total = s2[n, z].astype(F32)
        for k in range(7):
            total = total + got_z[n, k].astype(F32)
        out[...] = total * scale

    b_r.wait_recv()
    own[1] = own[1] + got_b[0].astype(F32)
    b_l.wait_recv()
    own[0] = own[0] + got_b[1].astype(F32)
    c_r.wait_recv()
    ig_out[0:half] = (own[0] + got_c[0].astype(F32)).astype(BF)
    c_l.wait_recv()
    ig_out[half : 2 * half] = (own[1] + got_c[1].astype(F32)).astype(BF)

    for copy in [a_r, a_l, b_r, b_l, c_r, c_l, sm_copy, *sm_ys, *sm_zs, *w_copies]:
        copy.wait_send()
    for copies in y_copies + z_copies:
        for copy in copies:
            copy.wait_send()


def back(scale, x, g, gb, mx, wv, wg, sm):
    dma = pltpu.SemaphoreType.DMA
    vmem = pl.BlockSpec(memory_space=pltpu.VMEM)
    return pl.pallas_call(
        functools.partial(back_kernel, scale),
        out_shape=(
            jax.ShapeDtypeStruct((1024, 512), BF),
            jax.ShapeDtypeStruct((32, 256), F32),
            jax.ShapeDtypeStruct((32, 256), F32),
            jax.ShapeDtypeStruct((32, 256), F32),
            jax.ShapeDtypeStruct((40, 256), F32),
        ),
        in_specs=[vmem] * 7,
        out_specs=(vmem,) * 5,
        scratch_shapes=[
            pltpu.VMEM((3, 2, 512, 512), BF),
            pltpu.VMEM((2, 512, 512), F32),
            pltpu.VMEM((2, 512, 512), BF),
            pltpu.VMEM((2, 512, 512), BF),
            pltpu.VMEM((2, 512, 512), BF),
            pltpu.VMEM((3, 32, 2, 32, 256), BF),
            pltpu.VMEM((3, 32, 32, 256), BF),
            pltpu.VMEM((3, 8, 4, 32, 256), BF),
            pltpu.VMEM((3, 3, 8, 32, 256), BF),
            pltpu.VMEM((3, 8, 32, 256), BF),
            pltpu.VMEM((3, 7, 32, 256), BF),
            pltpu.VMEM((2, 40, 256), F32),
            pltpu.VMEM((40, 256), F32),
            pltpu.VMEM((3, 40, 256), F32),
            pltpu.VMEM((7, 40, 256), F32),
            dma((6,)), dma((6,)), dma((3,)), dma((3,)), dma((3, 3)), dma((3, 3)),
            dma((3, 7)), dma((3, 7)), dma((11,)), dma((11,)),
        ],
        compiler_params=pltpu.CompilerParams(
            collective_id=0, has_side_effects=True, vmem_limit_bytes=60 * 1024 * 1024
        ),
        cost_estimate=pl.CostEstimate(
            flops=8_000_000_000, bytes_accessed=16_000_000, transcendentals=0
        ),
    )(x, g, gb, mx, wv, wg, sm)


def shards(block_input, out_grad, w_value, w_gate, conv_taps, norm_gain, norm_shift, w_proj):
    tok_rows = block_input.shape[0]
    kernel_len = conv_taps.shape[0]
    reach_back = kernel_len - 1
    channels_dev = w_value.shape[1]
    loss_scale = 1.0 / math.sqrt(tok_rows * lax.axis_size(SP))
    value_proj = jnp.dot(block_input, w_value, preferred_element_type=jnp.float32).astype(
        jnp.bfloat16
    )
    gate_proj = jnp.dot(block_input, w_gate, preferred_element_type=jnp.float32).astype(
        jnp.bfloat16
    )
    gate_sigmoid = jax.nn.sigmoid(gate_proj.astype(jnp.float32))
    value_wide = value_proj.astype(jnp.float32)
    gated_input = (value_wide * gate_sigmoid).astype(jnp.bfloat16)
    earlier = from_behind(gated_input[tok_rows - reach_back :], SP, 1)
    extended = jnp.concatenate([earlier, gated_input], axis=0).astype(jnp.float32)
    filtered = jnp.zeros((tok_rows, channels_dev), jnp.float32)
    for tap_index in range(kernel_len):
        begin = reach_back - tap_index
        filtered = filtered + conv_taps[tap_index] * extended[begin : begin + tok_rows]
    row_sum, row_square = together(
        (jnp.sum(filtered, axis=1), jnp.sum(filtered * filtered, axis=1)), "tp"
    )
    row_mean = row_sum / CH
    row_var = row_square / CH - row_mean * row_mean
    row_scale = lax.rsqrt(row_var + EPS)
    normed = (filtered - row_mean[:, None]) * row_scale[:, None]
    activated = normed * norm_gain + norm_shift
    act_sigmoid = jax.nn.sigmoid(activated)
    mixer_out = (activated * act_sigmoid).astype(jnp.bfloat16)
    grad_mixed = right_product(out_grad, w_proj)
    grad_act = grad_mixed * act_sigmoid * (1.0 + activated * (1.0 - act_sigmoid))
    grad_normed = grad_act * norm_gain
    back_sum, back_cross = together(
        (jnp.sum(grad_normed, axis=1), jnp.sum(grad_normed * normed, axis=1)), "tp"
    )
    grad_filtered = row_scale[:, None] * (
        grad_normed - back_sum[:, None] / CH - normed * (back_cross[:, None] / CH)
    )
    gain_part = jnp.sum(grad_act * normed, axis=0)
    shift_part = jnp.sum(grad_act, axis=0)
    padded_grad = jnp.pad(grad_filtered, ((reach_back, reach_back), (0, 0)))
    grad_extended = jnp.zeros((tok_rows + reach_back, channels_dev), jnp.float32)
    taps_rows = []
    for tap_index in range(kernel_len):
        begin = reach_back - tap_index
        grad_extended = (
            grad_extended
            + conv_taps[tap_index] * padded_grad[tap_index : tap_index + tok_rows + reach_back]
        )
        taps_rows.append(jnp.sum(grad_filtered * extended[begin : begin + tok_rows], axis=0))
    taps_part = jnp.stack(taps_rows, axis=0)
    returned = from_behind(grad_extended[:reach_back], SP, -1)
    grad_glu = jnp.concatenate(
        [grad_extended[reach_back:tok_rows], grad_extended[tok_rows:] + returned], axis=0
    )
    grad_value = (grad_glu * gate_sigmoid).astype(jnp.bfloat16)
    grad_gate = (grad_glu * value_wide * gate_sigmoid * (1.0 - gate_sigmoid)).astype(jnp.bfloat16)
    grad_both = jnp.concatenate([grad_value, grad_gate], axis=1)
    small = jnp.concatenate(
        [taps_part, gain_part[None], shift_part[None], jnp.zeros((7, channels_dev), F32)], axis=0
    )
    input_grad, value_wgrad, gate_wgrad, proj_rows, sums = back(
        loss_scale, block_input, out_grad, grad_both, mixer_out, w_value, w_gate, small
    )
    return (
        input_grad,
        value_wgrad,
        gate_wgrad,
        proj_rows.T,
        sums[:kernel_len],
        sums[kernel_len],
        sums[kernel_len + 1],
    )


def solution(mesh):
    return jax.shard_map(
        shards,
        mesh=mesh,
        in_specs=(
            P(SP, None),
            P(SP, None),
            P(None, "tp"),
            P(None, "tp"),
            P(None, "tp"),
            P("tp"),
            P("tp"),
            P("tp", None),
        ),
        out_specs=(
            P(SP, "tp"),
            P(SP, "tp"),
            P(SP, "tp"),
            P("tp", SP),
            P(None, "tp"),
            P("tp"),
            P("tp"),
        ),
        check_vma=False,
    )
```

```python
import functools
import math

import jax
import jax.numpy as jnp
from jax import lax
from jax.experimental import pallas as pl
from jax.experimental.pallas import tpu as pltpu
from jax.sharding import PartitionSpec as P

CH = 1024
SP = "sp"
MESH = pl.DeviceIdType.MESH
BF = jnp.bfloat16
F32 = jnp.float32
EPS = 0.05
TAPS = 31
T = 256
TILES = 4
R = 64


def plain(left, right):
    return jnp.dot(left, right, preferred_element_type=F32)


def rows_product(left, right):
    return lax.dot_general(left, right, (((1,), (1,)), ((), ())), preferred_element_type=F32)


def cols_product(left, right):
    return lax.dot_general(left, right, (((0,), (0,)), ((), ())), preferred_element_type=F32)


def loop(count, body):
    def step(i, carry):
        body(i)
        return carry

    lax.fori_loop(0, count, step, 0)


def whole(
    scale,
    x_h, g_h, wv_h, wg_h, taps, gain, shift, wp_h,
    ig_out, w_out, sm_out,
    x, g, wv, wg, wp, load,
    gi, gi_halo, vf, sg, filt, gm, gf, gf_halo, gb, mx, tg, gs,
    stc, wide, col_a, col_b, st1, got1, st2, got2,
    part, own, got_a, got_b, got_c,
    wbuf, got_w, s1, got_y, s2, got_z,
    smb, sm_c, sm_y, sm_z,
    hs, hr, t1s, t1r, t2s, t2r, as_, ar, bs, br, cs, cr,
    ws, wr, ys, yr, zs, zr, ms, mr,
):
    s = lax.axis_index(SP)
    t = lax.axis_index("tp")
    c, y, z = s % 2, (s // 2) % 4, s // 8
    right, left, far = (t + 1) % 4, (t + 3) % 4, (t + 2) % 4
    last_sp = 63

    def local(src, dst, k):
        return pltpu.make_async_copy(src, dst, load.at[k])

    def x_rows(i):
        rows = pl.ds(i * T, T)
        return local(x_h.at[rows], x.at[rows], i)

    loads = [local(wv_h, wv, 4), local(wg_h, wg, 5)]
    loads[0].start()
    x_rows(3).start()
    loads[1].start()
    for i in range(3):
        x_rows(i).start()
    late = [local(wp_h, wp, 6), local(g_h, g, 7)]
    for copy in late:
        copy.start()

    def at_y(k):
        return {SP: (z * 4 + (y + k) % 4) * 2 + c}

    def at_z(k):
        return {SP: (((z + k) % 8) * 4 + y) * 2 + c}

    def at_t(k):
        return {"tp": (t + k) % 4}

    partner = {SP: s + 1 - 2 * c}
    after = {SP: (s + 1) % 64}
    before = {SP: (s + 63) % 64}
    peers = [at_t(k) for k in (1, 2, 3)] + [partner, after, before]
    peers += [at_y(k) for k in (1, 2, 3)] + [at_z(k) for k in range(1, 8)]
    barrier = pltpu.get_barrier_semaphore()
    for peer in peers:
        pl.semaphore_signal(barrier, inc=1, device_id=peer, device_id_type=MESH)

    def remote(src, dst, ssem, rsem, device):
        return pltpu.make_async_remote_copy(
            src_ref=src, dst_ref=dst, send_sem=ssem, recv_sem=rsem,
            device_id=device, device_id_type=MESH,
        )

    lane = lax.broadcasted_iota(jnp.int32, (R, 128), 1)
    tg[...] = jnp.zeros_like(tg)
    gs[...] = jnp.zeros_like(gs)
    wide[...] = jnp.zeros_like(wide)

    halo_send = remote(gi.at[:, pl.ds(1024, 32)], gi_halo, hs.at[0], hr.at[0], after)
    grad_send = remote(gf.at[:, pl.ds(0, 32)], gf_halo, hs.at[1], hr.at[1], before)

    def st1_send(i, k):
        return remote(st1.at[i], got1.at[i, k - 1], t1s.at[i, k - 1], t1r.at[i, k - 1], at_t(k))

    def st2_send(i, k):
        return remote(st2.at[i], got2.at[i, k - 1], t2s.at[i, k - 1], t2r.at[i, k - 1], at_t(k))

    def project(i):
        rows = pl.ds(pl.multiple_of(i * T, T), T)
        x_rows(i).wait()
        value = plain(x[rows, :], wv[...]).astype(BF).astype(F32)
        gate = plain(x[rows, :], wg[...]).astype(BF).astype(F32)
        sig = jax.nn.sigmoid(gate)
        gated = (value * sig).astype(BF).astype(F32)
        at = pl.ds(pl.multiple_of(i * T + 32, 32), T)
        for h in range(2):
            lanes = slice(h * 128, h * 128 + 128)
            vf[h, rows, :] = value[:, lanes]
            sg[h, rows, :] = sig[:, lanes]
            gi[h, at, :] = gated[:, lanes]

    for copy in loads:
        copy.wait()
    project(3)
    pl.semaphore_wait(barrier, len(peers))
    halo_send.start()
    loop(3, project)
    halo_send.wait_recv()
    gi[:, 0:32, :] = jnp.where(s == 0, 0.0, gi_halo[...])

    def filter_tile(i):
        def block(b):
            base = pl.multiple_of(i * T + b * R, R)
            out = []
            for h in range(2):
                acc = jnp.zeros((R, 128), F32)
                for k in range(TAPS):
                    tap = taps[k : k + 1, h * 128 : h * 128 + 128]
                    acc = acc + tap * gi[h, pl.ds(base + 32 - k, R), :]
                filt[h, pl.ds(base, R), :] = acc
                out.append(acc)
            total = jnp.sum(out[0] + out[1], axis=1, keepdims=True)
            square = jnp.sum(out[0] * out[0] + out[1] * out[1], axis=1, keepdims=True)
            stc[pl.ds(pl.multiple_of(b * R, R), R), :] = jnp.where(
                lane == 0, total, jnp.where(lane == 1, square, 0.0)
            )

        loop(T // R, block)
        st1[i] = stc[...].T[0:8, :]
        for k in (1, 2, 3):
            st1_send(i, k).start()

    loop(TILES, filter_tile)

    for copy in late:
        copy.wait()

    def mixed(i):
        rows = pl.ds(pl.multiple_of(i * T, T), T)
        out = rows_product(g[rows, :], wp[...])
        for h in range(2):
            gm[h, rows, :] = out[:, h * 128 : h * 128 + 128]

    loop(TILES, mixed)

    def activate(i):
        for k in (1, 2, 3):
            st1_send(i, k).wait_recv()
        sums = st1[i] + got1[i, 0] + got1[i, 1] + got1[i, 2]
        mean = sums[0:1] / CH
        var = sums[1:2] / CH - mean * mean
        wide[0:1, :] = mean
        wide[1:2, :] = lax.rsqrt(var + EPS)
        col_a[i] = wide[...].T

        def block(b):
            local_rows = pl.ds(pl.multiple_of(b * R, R), R)
            rows = pl.ds(pl.multiple_of(i * T + b * R, R), R)
            mean = col_a[i, local_rows, 0:1]
            inv = col_a[i, local_rows, 1:2]
            first, second = 0.0, 0.0
            for h in range(2):
                lanes = slice(h * 128, h * 128 + 128)
                normed = (filt[h, rows, :] - mean) * inv
                act = normed * gain[0:1, lanes] + shift[0:1, lanes]
                sig = jax.nn.sigmoid(act)
                mx[rows, lanes] = (act * sig).astype(BF)
                grad = gm[h, rows, :] * sig * (1.0 + act * (1.0 - sig))
                gs[0, h] = gs[0, h] + (grad * normed).reshape(R // 8, 8, 128).sum(axis=0)
                gs[1, h] = gs[1, h] + grad.reshape(R // 8, 8, 128).sum(axis=0)
                grad = grad * gain[0:1, lanes]
                filt[h, rows, :] = normed
                gm[h, rows, :] = grad
                first = first + grad
                second = second + grad * normed
            first = jnp.sum(first, axis=1, keepdims=True)
            second = jnp.sum(second, axis=1, keepdims=True)
            stc[local_rows, :] = jnp.where(lane == 0, first, jnp.where(lane == 1, second, 0.0))

        loop(T // R, block)
        st2[i] = stc[...].T[0:8, :]
        for k in (1, 2, 3):
            st2_send(i, k).start()

    loop(TILES, activate)

    def pair_send(n):
        return remote(wbuf.at[n, :, 1 - c], got_w.at[n], ws.at[n], wr.at[n], partner)

    def y_send(n, k):
        return remote(
            s1.at[n, :, (y + k) % 4], got_y.at[n, k - 1], ys.at[n, k - 1], yr.at[n, k - 1], at_y(k)
        )

    def z_send(n, k):
        return remote(
            s2.at[n, (z + k) % 8], got_z.at[n, k - 1], zs.at[n, k - 1], zr.at[n, k - 1], at_z(k)
        )

    def weight_chunk(n):
        source, other, off = (g, mx, 0) if n == 0 else (x, gb, (n - 1) * 256)

        def tile(zb):
            span = pl.ds(pl.multiple_of(zb * 256, 256), 256)
            out = cols_product(source[:, span], other[:, off : off + 256])
            wbuf[n, pl.ds(zb * 4, 4)] = out.astype(BF).reshape(4, 2, 32, 256)

        loop(8, tile)
        pair_send(n).start()

    def pair_sum(n):
        pair_send(n).wait_recv()

        def tile(zb):
            rows = pl.ds(zb * 4, 4)
            s1[n, zb] = (wbuf[n, rows, c].astype(F32) + got_w[n, rows].astype(F32)).astype(BF)

        loop(8, tile)
        for k in (1, 2, 3):
            y_send(n, k).start()

    def y_sum(n):
        for k in (1, 2, 3):
            y_send(n, k).wait_recv()
        total = s1[n, :, y].astype(F32)
        for k in range(3):
            total = total + got_y[n, k].astype(F32)
        s2[n] = total.astype(BF)
        for k in range(1, 8):
            z_send(n, k).start()

    def z_sum(n):
        for k in range(1, 8):
            z_send(n, k).wait_recv()
        total = s2[n, z].astype(F32)
        for k in range(7):
            total = total + got_z[n, k].astype(F32)
        w_out[n] = total * scale

    weight_chunk(0)

    def filtered_grad(i):
        for k in (1, 2, 3):
            st2_send(i, k).wait_recv()
        sums = (st2[i] + got2[i, 0] + got2[i, 1] + got2[i, 2]) / CH
        wide[0:2, :] = sums[0:2]
        col_b[...] = wide[...].T

        def block(b):
            local_rows = pl.ds(pl.multiple_of(b * R, R), R)
            rows = pl.ds(pl.multiple_of(i * T + b * R, R), R)
            inv = col_a[i, local_rows, 1:2]
            m1 = col_b[local_rows, 0:1]
            m2 = col_b[local_rows, 1:2]
            for h in range(2):
                gf[h, rows, :] = inv * (gm[h, rows, :] - m1 - filt[h, rows, :] * m2)

        loop(T // R, block)

    filtered_grad(0)
    grad_send.start()
    loop(TILES - 1, lambda i: filtered_grad(i + 1))
    pair_sum(0)
    grad_send.wait_recv()
    gf[:, 1024:1056, :] = jnp.where(s == last_sp, 0.0, gf_halo[...])

    def toward(i):
        first = i < TILES // 2
        return jnp.where(first, right, left), jnp.where(first, left, right)

    def a_send(i):
        return remote(part.at[0, i], got_a.at[i], as_.at[i], ar.at[i], {"tp": toward(i)[0]})

    def b_send(i):
        return remote(part.at[1, i], got_b.at[i], bs.at[i], br.at[i], {"tp": toward(i)[1]})

    def c_send(i):
        return remote(part.at[2, i], got_c.at[i], cs.at[i], cr.at[i], {"tp": toward(i)[0]})

    def back_tile(i):
        for h in range(2):
            lanes = slice(h * 128, h * 128 + 128)
            lanes_g = slice(256 + h * 128, 384 + h * 128)

            def block(b, h=h, lanes=lanes, lanes_g=lanes_g):
                base = pl.multiple_of(i * T + b * R, R)
                rows = pl.ds(base, R)
                gated = gi[h, pl.ds(pl.multiple_of(base + 32, 32), R), :]
                acc = jnp.zeros((R, 128), F32)
                for k in range(TAPS):
                    moved = gf[h, pl.ds(base + k, R), :]
                    acc = acc + taps[k : k + 1, lanes] * moved
                    tg[h, k] = tg[h, k] + (gated * moved).reshape(R // 8, 8, 128).sum(axis=0)
                sig = sg[h, rows, :]
                gv = acc * sig
                gb[rows, lanes] = gv.astype(BF)
                gb[rows, lanes_g] = (gv * vf[h, rows, :] * (1.0 - sig)).astype(BF)

            loop(T // R, block)

        rows = pl.ds(pl.multiple_of(i * T, T), T)

        def partial(block):
            span = pl.ds(pl.multiple_of(block * 512, 512), 512)
            return rows_product(gb[rows, 0:256], wv[span, :]) + rows_product(
                gb[rows, 256:512], wg[span, :]
            )

        near, back = toward(i)
        part[0, i] = partial(far).astype(BF)
        a_send(i).start()
        part[1, i] = partial(back).astype(BF)
        b_send(i).start()
        part[2, i] = partial(near).astype(BF)
        own[i] = partial(t)

    loop(TILES, back_tile)

    def combine(i):
        a_send(i).wait_recv()
        part[2, i] = (part[2, i].astype(F32) + got_a[i].astype(F32)).astype(BF)
        c_send(i).start()

    for h in range(2):
        lanes = slice(h * 128, h * 128 + 128)
        smb[0, 0:TAPS, lanes] = jnp.sum(tg[h], axis=1)
        smb[0, 31:32, lanes] = jnp.sum(gs[0, h], axis=0, keepdims=True)
        smb[0, 32:33, lanes] = jnp.sum(gs[1, h], axis=0, keepdims=True)
    smb[0, 33:40, :] = jnp.zeros((7, 256), F32)
    sm_pair = remote(smb.at[0], sm_c, ms.at[0], mr.at[0], partner)
    sm_pair.start()

    combine(0)
    weight_chunk(1)
    y_sum(0)
    sm_pair.wait_recv()
    smb[1] = smb[0] + sm_c[...]
    sm_ys = [remote(smb.at[1], sm_y.at[k - 1], ms.at[k], mr.at[k], at_y(k)) for k in (1, 2, 3)]
    for copy in sm_ys:
        copy.start()
    pair_sum(1)
    combine(1)
    weight_chunk(2)
    pair_sum(2)
    for copy in sm_ys:
        copy.wait_recv()
    smb[2] = smb[1] + sm_y[0] + sm_y[1] + sm_y[2]
    sm_zs = [
        remote(smb.at[2], sm_z.at[k - 1], ms.at[3 + k], mr.at[3 + k], at_z(k)) for k in range(1, 8)
    ]
    for copy in sm_zs:
        copy.start()
    y_sum(1)
    y_sum(2)
    combine(2)
    combine(3)
    z_sum(0)
    for copy in sm_zs:
        copy.wait_recv()
    total = smb[2]
    for k in range(7):
        total = total + sm_z[k]
    sm_out[...] = total * scale
    z_sum(1)
    z_sum(2)

    def finish(i):
        b_send(i).wait_recv()
        c_send(i).wait_recv()
        rows = pl.ds(pl.multiple_of(i * T, T), T)
        ig_out[rows, :] = (own[i] + got_b[i].astype(F32) + got_c[i].astype(F32)).astype(BF)

    loop(TILES, finish)

    halo_send.wait_send()
    grad_send.wait_send()
    for copy in [sm_pair, *sm_ys, *sm_zs]:
        copy.wait_send()
    for n in range(3):
        pair_send(n).wait_send()
        for k in (1, 2, 3):
            y_send(n, k).wait_send()
        for k in range(1, 8):
            z_send(n, k).wait_send()

    def drain(i):
        for k in (1, 2, 3):
            st1_send(i, k).wait_send()
            st2_send(i, k).wait_send()
        a_send(i).wait_send()
        b_send(i).wait_send()
        c_send(i).wait_send()

    loop(TILES, drain)


def module(scale, x, g, wv, wg, taps, gain, shift, wp):
    dma = pltpu.SemaphoreType.DMA
    vmem = pl.BlockSpec(memory_space=pltpu.VMEM)
    hbm = pl.BlockSpec(memory_space=pl.ANY)

    def half(rows, kind=F32):
        return pltpu.VMEM((2, rows, 128), kind)

    tile = pltpu.VMEM((TILES, T, 512), BF)
    return pl.pallas_call(
        functools.partial(whole, scale),
        out_shape=(
            jax.ShapeDtypeStruct((1024, 512), BF),
            jax.ShapeDtypeStruct((3, 32, 256), F32),
            jax.ShapeDtypeStruct((40, 256), F32),
        ),
        in_specs=[hbm, hbm, hbm, hbm, vmem, vmem, vmem, hbm],
        out_specs=(vmem,) * 3,
        scratch_shapes=[
            pltpu.VMEM((1024, 2048), BF), pltpu.VMEM((1024, 2048), BF),
            pltpu.VMEM((2048, 256), BF), pltpu.VMEM((2048, 256), BF), pltpu.VMEM((256, 2048), BF),
            dma((8,)),
            half(1056), half(32), half(1024), half(1024), half(1024), half(1024), half(1056), half(32),
            pltpu.VMEM((1024, 512), BF), pltpu.VMEM((1024, 256), BF),
            pltpu.VMEM((2, TAPS, 8, 128), F32), pltpu.VMEM((2, 2, 8, 128), F32),
            pltpu.VMEM((T, 128), F32), pltpu.VMEM((128, T), F32),
            pltpu.VMEM((TILES, T, 128), F32), pltpu.VMEM((T, 128), F32),
            pltpu.VMEM((TILES, 8, T), F32), pltpu.VMEM((TILES, 3, 8, T), F32),
            pltpu.VMEM((TILES, 8, T), F32), pltpu.VMEM((TILES, 3, 8, T), F32),
            pltpu.VMEM((3, TILES, T, 512), BF), pltpu.VMEM((TILES, T, 512), F32),
            tile, tile, tile,
            pltpu.VMEM((3, 32, 2, 32, 256), BF), pltpu.VMEM((3, 32, 32, 256), BF),
            pltpu.VMEM((3, 8, 4, 32, 256), BF), pltpu.VMEM((3, 3, 8, 32, 256), BF),
            pltpu.VMEM((3, 8, 32, 256), BF), pltpu.VMEM((3, 7, 32, 256), BF),
            pltpu.VMEM((3, 40, 256), F32), pltpu.VMEM((40, 256), F32),
            pltpu.VMEM((3, 40, 256), F32), pltpu.VMEM((7, 40, 256), F32),
            dma((2,)), dma((2,)),
            dma((TILES, 3)), dma((TILES, 3)), dma((TILES, 3)), dma((TILES, 3)),
            dma((TILES,)), dma((TILES,)), dma((TILES,)), dma((TILES,)), dma((TILES,)), dma((TILES,)),
            dma((3,)), dma((3,)), dma((3, 3)), dma((3, 3)), dma((3, 7)), dma((3, 7)),
            dma((11,)), dma((11,)),
        ],
        compiler_params=pltpu.CompilerParams(
            collective_id=0, has_side_effects=True, vmem_limit_bytes=62 * 1024 * 1024
        ),
        cost_estimate=pl.CostEstimate(
            flops=10_000_000_000, bytes_accessed=14_000_000, transcendentals=1_000_000
        ),
    )(x, g, wv, wg, taps, gain, shift, wp)


def placed(ig, w, sm, ig_out, v_out, g_out, p_out, t_out, gain_out, shift_out):
    ig_out[...] = ig[...]
    v_out[...] = w[1]
    g_out[...] = w[2]
    p_out[...] = w[0].T
    t_out[...] = sm[0:TAPS]
    gain_out[...] = sm[TAPS : TAPS + 1]
    shift_out[...] = sm[TAPS + 1 : TAPS + 2]


def shards(block_input, out_grad, w_value, w_gate, conv_taps, norm_gain, norm_shift, w_proj):
    loss_scale = 1.0 / math.sqrt(block_input.shape[0] * lax.axis_size(SP))
    parts = module(
        loss_scale, block_input, out_grad, w_value, w_gate, conv_taps,
        norm_gain.reshape(1, -1), norm_shift.reshape(1, -1), w_proj,
    )
    shapes = [
        ((1024, 512), BF), ((32, 256), F32), ((32, 256), F32), ((256, 32), F32),
        ((TAPS, 256), F32), ((1, 256), F32), ((1, 256), F32),
    ]
    out = pl.pallas_call(
        placed,
        out_shape=tuple(jax.ShapeDtypeStruct(*shape) for shape in shapes),
        cost_estimate=pl.CostEstimate(flops=1_000_000, bytes_accessed=2_000_000, transcendentals=0),
    )(*parts)
    return (*out[:5], out[5].reshape(-1), out[6].reshape(-1))


def solution(mesh):
    return jax.shard_map(
        shards,
        mesh=mesh,
        in_specs=(
            P(SP, None),
            P(SP, None),
            P(None, "tp"),
            P(None, "tp"),
            P(None, "tp"),
            P("tp"),
            P("tp"),
            P("tp", None),
        ),
        out_specs=(
            P(SP, "tp"),
            P(SP, "tp"),
            P(SP, "tp"),
            P("tp", SP),
            P(None, "tp"),
            P("tp"),
            P("tp"),
        ),
        check_vma=False,
    )
```

```python
import functools
import math

import jax
import jax.numpy as jnp
from jax import lax
from jax.experimental import pallas as pl
from jax.experimental.pallas import tpu as pltpu
from jax.sharding import PartitionSpec as P

CH = 1024
SP = "sp"
MESH = pl.DeviceIdType.MESH
BF = jnp.bfloat16
F32 = jnp.float32
EPS = 0.05
TAPS = 31
T = 256
TILES = 4
R = 64


def plain(left, right):
    return jnp.dot(left, right, preferred_element_type=F32)


def rows_product(left, right):
    return lax.dot_general(left, right, (((1,), (1,)), ((), ())), preferred_element_type=F32)


def cols_product(left, right):
    return lax.dot_general(left, right, (((0,), (0,)), ((), ())), preferred_element_type=F32)


def logistic(v):
    return 0.5 * jnp.tanh(0.5 * v) + 0.5


def loop(count, body):
    def step(i, carry):
        body(i)
        return carry

    lax.fori_loop(0, count, step, 0)


def whole(
    scale,
    x_h, g_h, wv_h, wg_h, taps, gain, shift, wp_h,
    ig_out, w_out, sm_out,
    x, g, wv, wg, wp, load,
    gi, gi_halo, vf, sg, filt, gm, gf, gf_halo, gb, mx, tg, gs,
    sum_a, sum_b, col_m, col_i, col_a, col_b, st1, got1, st2, got2,
    part, own, got_a, got_b, got_c,
    wbuf, got_w, s1, got_y, s2, got_z,
    smb, sm_c, sm_y, sm_z,
    hs, hr, t1s, t1r, t2s, t2r, as_, ar, bs, br, cs, cr,
    ws, wr, ys, yr, zs, zr, ms, mr,
):
    s = lax.axis_index(SP)
    t = lax.axis_index("tp")
    c, y, z = s % 2, (s // 2) % 4, s // 8
    right, left, far = (t + 1) % 4, (t + 3) % 4, (t + 2) % 4
    last_sp = 63

    def local(src, dst, k):
        return pltpu.make_async_copy(src, dst, load.at[k])

    def x_rows(i):
        rows = pl.ds(i * T, T)
        return local(x_h.at[rows], x.at[rows], i)

    loads = [local(wv_h, wv, 4), local(wg_h, wg, 5)]
    loads[0].start()
    x_rows(3).start()
    loads[1].start()
    for i in range(3):
        x_rows(i).start()
    late = [local(wp_h, wp, 6), local(g_h, g, 7)]
    for copy in late:
        copy.start()

    def at_y(k):
        return {SP: (z * 4 + (y + k) % 4) * 2 + c}

    def at_z(k):
        return {SP: (((z + k) % 8) * 4 + y) * 2 + c}

    def at_t(k):
        return {"tp": (t + k) % 4}

    partner = {SP: s + 1 - 2 * c}
    after = {SP: (s + 1) % 64}
    before = {SP: (s + 63) % 64}
    peers = [at_t(k) for k in (1, 2, 3)] + [partner, after, before]
    peers += [at_y(k) for k in (1, 2, 3)] + [at_z(k) for k in range(1, 8)]
    barrier = pltpu.get_barrier_semaphore()
    for peer in peers:
        pl.semaphore_signal(barrier, inc=1, device_id=peer, device_id_type=MESH)

    def remote(src, dst, ssem, rsem, device):
        return pltpu.make_async_remote_copy(
            src_ref=src, dst_ref=dst, send_sem=ssem, recv_sem=rsem,
            device_id=device, device_id_type=MESH,
        )

    tg[...] = jnp.zeros_like(tg)
    gs[...] = jnp.zeros_like(gs)
    st1[...] = jnp.zeros_like(st1)
    st2[...] = jnp.zeros_like(st2)

    def token_sums(tile):
        return jnp.sum(tile[...].T, axis=0, keepdims=True)

    def over_lanes(row):
        return jnp.broadcast_to(row, (128, T)).T


    halo_send = remote(gi.at[:, pl.ds(1024, 32)], gi_halo, hs.at[0], hr.at[0], after)
    grad_send = remote(gf.at[:, pl.ds(0, 32)], gf_halo, hs.at[1], hr.at[1], before)

    def st1_send(i, k):
        return remote(st1.at[i], got1.at[i, k - 1], t1s.at[i, k - 1], t1r.at[i, k - 1], at_t(k))

    def st2_send(i, k):
        return remote(st2.at[i], got2.at[i, k - 1], t2s.at[i, k - 1], t2r.at[i, k - 1], at_t(k))

    def project(i):
        rows = pl.ds(pl.multiple_of(i * T, T), T)
        x_rows(i).wait()
        value = plain(x[rows, :], wv[...]).astype(BF).astype(F32)
        gate = plain(x[rows, :], wg[...]).astype(BF).astype(F32)
        sig = logistic(gate)
        gated = (value * sig).astype(BF).astype(F32)
        at = pl.ds(pl.multiple_of(i * T + 32, 32), T)
        for h in range(2):
            lanes = slice(h * 128, h * 128 + 128)
            vf[h, rows, :] = value[:, lanes]
            sg[h, rows, :] = sig[:, lanes]
            gi[h, at, :] = gated[:, lanes]

    def filter_tile(i):
        def block(b):
            base = pl.multiple_of(i * T + b * 128, 128)
            rows = pl.ds(base, 128)
            tile = pl.ds(pl.multiple_of(b * 128, 128), 128)
            for h in range(2):
                acc = jnp.zeros((128, 128), F32)
                for k in range(TAPS):
                    tap = taps[k : k + 1, h * 128 : h * 128 + 128]
                    acc = acc + tap * gi[h, pl.ds(base + 32 - k, 128), :]
                filt[h, rows, :] = acc
                if h == 0:
                    sum_a[tile, :] = acc
                    sum_b[tile, :] = acc * acc
                else:
                    sum_a[tile, :] = sum_a[tile, :] + acc
                    sum_b[tile, :] = sum_b[tile, :] + acc * acc

        loop(T // 128, block)
        st1[i, 0:1] = token_sums(sum_a)
        st1[i, 1:2] = token_sums(sum_b)
        for k in (1, 2, 3):
            st1_send(i, k).start()

    def mixed(i):
        rows = pl.ds(pl.multiple_of(i * T, T), T)
        out = rows_product(g[rows, :], wp[...])
        for h in range(2):
            gm[h, rows, :] = out[:, h * 128 : h * 128 + 128]

    def activate(i):
        for k in (1, 2, 3):
            st1_send(i, k).wait_recv()
        sums = st1[i] + got1[i, 0] + got1[i, 1] + got1[i, 2]
        mean = sums[0:1] / CH
        var = sums[1:2] / CH - mean * mean
        col_m[i] = over_lanes(mean)
        col_i[i] = over_lanes(lax.rsqrt(var + EPS))

        def block(b):
            local_rows = pl.ds(pl.multiple_of(b * R, R), R)
            rows = pl.ds(pl.multiple_of(i * T + b * R, R), R)
            mean = col_m[i, local_rows, :]
            inv = col_i[i, local_rows, :]
            first, second = 0.0, 0.0
            for h in range(2):
                lanes = slice(h * 128, h * 128 + 128)
                normed = (filt[h, rows, :] - mean) * inv
                act = normed * gain[0:1, lanes] + shift[0:1, lanes]
                sig = logistic(act)
                mx[rows, lanes] = (act * sig).astype(BF)
                grad = gm[h, rows, :] * sig * (1.0 + act * (1.0 - sig))
                gs[0, h] = gs[0, h] + (grad * normed).reshape(R // 8, 8, 128).sum(axis=0)
                gs[1, h] = gs[1, h] + grad.reshape(R // 8, 8, 128).sum(axis=0)
                grad = grad * gain[0:1, lanes]
                filt[h, rows, :] = normed
                gm[h, rows, :] = grad
                first = first + grad
                second = second + grad * normed
            sum_a[local_rows, :] = first
            sum_b[local_rows, :] = second

        loop(T // R, block)
        st2[i, 0:1] = token_sums(sum_a)
        st2[i, 1:2] = token_sums(sum_b)
        for k in (1, 2, 3):
            st2_send(i, k).start()

    def pair_send(n):
        return remote(wbuf.at[n, :, 1 - c], got_w.at[n], ws.at[n], wr.at[n], partner)

    def y_send(n, k):
        return remote(
            s1.at[n, :, (y + k) % 4], got_y.at[n, k - 1], ys.at[n, k - 1], yr.at[n, k - 1], at_y(k)
        )

    def z_send(n, k):
        return remote(
            s2.at[n, (z + k) % 8], got_z.at[n, k - 1], zs.at[n, k - 1], zr.at[n, k - 1], at_z(k)
        )

    def proj_chunk():
        def tile(zb):
            span = pl.ds(pl.multiple_of(zb * 512, 512), 512)
            out = cols_product(g[:, span], mx[...]).astype(BF)
            wbuf[0, pl.ds(zb * 8, 8)] = out.reshape(8, 2, 32, 256)

        loop(4, tile)
        pair_send(0).start()

    def gate_chunks():
        def tile(zb):
            span = pl.ds(pl.multiple_of(zb * 512, 512), 512)
            out = cols_product(x[:, span], gb[...]).astype(BF)
            for n in (0, 1):
                wbuf[n + 1, pl.ds(zb * 8, 8)] = out[:, n * 256 : n * 256 + 256].reshape(8, 2, 32, 256)

        loop(4, tile)
        pair_send(1).start()
        pair_send(2).start()

    def pair_sum(n):
        pair_send(n).wait_recv()

        def tile(zb):
            rows = pl.ds(zb * 4, 4)
            s1[n, zb] = (wbuf[n, rows, c].astype(F32) + got_w[n, rows].astype(F32)).astype(BF)

        loop(8, tile)
        for k in (1, 2, 3):
            y_send(n, k).start()

    def y_sum(n):
        for k in (1, 2, 3):
            y_send(n, k).wait_recv()
        total = s1[n, :, y].astype(F32)
        for k in range(3):
            total = total + got_y[n, k].astype(F32)
        s2[n] = total.astype(BF)
        for k in range(1, 8):
            z_send(n, k).start()

    def z_sum(n):
        for k in range(1, 8):
            z_send(n, k).wait_recv()
        total = s2[n, z].astype(F32)
        for k in range(7):
            total = total + got_z[n, k].astype(F32)
        w_out[n] = total * scale

    def filtered_grad(i):
        for k in (1, 2, 3):
            st2_send(i, k).wait_recv()
        sums = (st2[i] + got2[i, 0] + got2[i, 1] + got2[i, 2]) / CH
        col_a[...] = over_lanes(sums[0:1])
        col_b[...] = over_lanes(sums[1:2])

        def block(b):
            local_rows = pl.ds(pl.multiple_of(b * R, R), R)
            rows = pl.ds(pl.multiple_of(i * T + b * R, R), R)
            inv = col_i[i, local_rows, :]
            m1 = col_a[local_rows, :]
            m2 = col_b[local_rows, :]
            for h in range(2):
                gf[h, rows, :] = inv * (gm[h, rows, :] - m1 - filt[h, rows, :] * m2)

        loop(T // R, block)

    def toward(i):
        first = i < TILES // 2
        return jnp.where(first, right, left), jnp.where(first, left, right)

    def a_send(i):
        return remote(part.at[0, i], got_a.at[i], as_.at[i], ar.at[i], {"tp": toward(i)[0]})

    def b_send(i):
        return remote(part.at[1, i], got_b.at[i], bs.at[i], br.at[i], {"tp": toward(i)[1]})

    def c_send(i):
        return remote(part.at[2, i], got_c.at[i], cs.at[i], cr.at[i], {"tp": toward(i)[0]})

    def back_tile(i):
        for h in range(2):
            lanes = slice(h * 128, h * 128 + 128)
            lanes_g = slice(256 + h * 128, 384 + h * 128)

            def block(b, h=h, lanes=lanes, lanes_g=lanes_g):
                base = pl.multiple_of(i * T + b * R, R)
                rows = pl.ds(base, R)
                gated = gi[h, pl.ds(pl.multiple_of(base + 32, 32), R), :]
                acc = jnp.zeros((R, 128), F32)
                for k in range(TAPS):
                    moved = gf[h, pl.ds(base + k, R), :]
                    acc = acc + taps[k : k + 1, lanes] * moved
                    tg[h, k] = tg[h, k] + (gated * moved).reshape(R // 8, 8, 128).sum(axis=0)
                sig = sg[h, rows, :]
                gv = acc * sig
                gb[rows, lanes] = gv.astype(BF)
                gb[rows, lanes_g] = (gv * vf[h, rows, :] * (1.0 - sig)).astype(BF)

            loop(T // R, block)

        rows = pl.ds(pl.multiple_of(i * T, T), T)

        def partial(block):
            span = pl.ds(pl.multiple_of(block * 512, 512), 512)
            return rows_product(gb[rows, 0:256], wv[span, :]) + rows_product(
                gb[rows, 256:512], wg[span, :]
            )

        near, back = toward(i)
        part[0, i] = partial(far).astype(BF)
        a_send(i).start()
        part[1, i] = partial(back).astype(BF)
        b_send(i).start()
        part[2, i] = partial(near).astype(BF)
        own[i] = partial(t)

    def combine(i):
        a_send(i).wait_recv()
        part[2, i] = (part[2, i].astype(F32) + got_a[i].astype(F32)).astype(BF)
        c_send(i).start()

    def pair(first, body):
        loop(2, lambda j: body(first + j))

    for copy in loads:
        copy.wait()
    project(3)
    pl.semaphore_wait(barrier, len(peers))
    halo_send.start()
    pair(0, project)
    halo_send.wait_recv()
    gi[:, 0:32, :] = jnp.where(s == 0, 0.0, gi_halo[...])
    pair(0, filter_tile)
    project(2)
    for copy in late:
        copy.wait()
    pair(0, mixed)
    pair(0, activate)
    pair(2, filter_tile)
    filtered_grad(0)
    grad_send.start()
    filtered_grad(1)
    back_tile(0)
    pair(2, mixed)
    pair(2, activate)

    def middle(j):
        @pl.when(j == 2)
        def _():
            proj_chunk()

        @pl.when(j < 3)
        def _():
            filtered_grad(j + 1)

        @pl.when(j == 3)
        def _():
            grad_send.wait_recv()
            gf[:, 1024:1056, :] = jnp.where(s == last_sp, 0.0, gf_halo[...])

        back_tile(j)

    loop(3, lambda j: middle(j + 1))

    for h in range(2):
        lanes = slice(h * 128, h * 128 + 128)
        smb[0, 0:TAPS, lanes] = jnp.sum(tg[h], axis=1)
        smb[0, 31:32, lanes] = jnp.sum(gs[0, h], axis=0, keepdims=True)
        smb[0, 32:33, lanes] = jnp.sum(gs[1, h], axis=0, keepdims=True)
    smb[0, 33:40, :] = jnp.zeros((7, 256), F32)
    sm_pair = remote(smb.at[0], sm_c, ms.at[0], mr.at[0], partner)
    sm_pair.start()
    pair_sum(0)
    gate_chunks()
    sm_pair.wait_recv()
    smb[1] = smb[0] + sm_c[...]
    sm_ys = [remote(smb.at[1], sm_y.at[k - 1], ms.at[k], mr.at[k], at_y(k)) for k in (1, 2, 3)]
    for copy in sm_ys:
        copy.start()
    loop(2, lambda j: pair_sum(j + 1))
    pair(0, combine)
    y_sum(0)
    for copy in sm_ys:
        copy.wait_recv()
    smb[2] = smb[1] + sm_y[0] + sm_y[1] + sm_y[2]
    sm_zs = [
        remote(smb.at[2], sm_z.at[k - 1], ms.at[3 + k], mr.at[3 + k], at_z(k)) for k in range(1, 8)
    ]
    for copy in sm_zs:
        copy.start()
    loop(2, lambda j: y_sum(j + 1))
    pair(2, combine)
    z_sum(0)
    for copy in sm_zs:
        copy.wait_recv()
    total = smb[2]
    for k in range(7):
        total = total + sm_z[k]
    sm_out[...] = total * scale
    loop(2, lambda j: z_sum(j + 1))

    def finish(i):
        b_send(i).wait_recv()
        c_send(i).wait_recv()
        rows = pl.ds(pl.multiple_of(i * T, T), T)
        ig_out[rows, :] = (own[i] + got_b[i].astype(F32) + got_c[i].astype(F32)).astype(BF)

    loop(TILES, finish)

    halo_send.wait_send()
    grad_send.wait_send()
    for copy in [sm_pair, *sm_ys, *sm_zs]:
        copy.wait_send()
    for n in range(3):
        pair_send(n).wait_send()
        for k in (1, 2, 3):
            y_send(n, k).wait_send()
        for k in range(1, 8):
            z_send(n, k).wait_send()

    def drain(i):
        for k in (1, 2, 3):
            st1_send(i, k).wait_send()
            st2_send(i, k).wait_send()
        a_send(i).wait_send()
        b_send(i).wait_send()
        c_send(i).wait_send()

    loop(TILES, drain)


def module(scale, x, g, wv, wg, taps, gain, shift, wp):
    dma = pltpu.SemaphoreType.DMA
    vmem = pl.BlockSpec(memory_space=pltpu.VMEM)
    hbm = pl.BlockSpec(memory_space=pl.ANY)

    def half(rows, kind=F32):
        return pltpu.VMEM((2, rows, 128), kind)

    tile = pltpu.VMEM((TILES, T, 512), BF)
    return pl.pallas_call(
        functools.partial(whole, scale),
        out_shape=(
            jax.ShapeDtypeStruct((1024, 512), BF),
            jax.ShapeDtypeStruct((3, 32, 256), F32),
            jax.ShapeDtypeStruct((40, 256), F32),
        ),
        in_specs=[hbm, hbm, hbm, hbm, vmem, vmem, vmem, hbm],
        out_specs=(vmem,) * 3,
        scratch_shapes=[
            pltpu.VMEM((1024, 2048), BF), pltpu.VMEM((1024, 2048), BF),
            pltpu.VMEM((2048, 256), BF), pltpu.VMEM((2048, 256), BF), pltpu.VMEM((256, 2048), BF),
            dma((8,)),
            half(1056), half(32), half(1024), half(1024), half(1024), half(1024), half(1056), half(32),
            pltpu.VMEM((1024, 512), BF), pltpu.VMEM((1024, 256), BF),
            pltpu.VMEM((2, TAPS, 8, 128), F32), pltpu.VMEM((2, 2, 8, 128), F32),
            pltpu.VMEM((T, 128), F32), pltpu.VMEM((T, 128), F32),
            pltpu.VMEM((TILES, T, 128), F32), pltpu.VMEM((TILES, T, 128), F32),
            pltpu.VMEM((T, 128), F32), pltpu.VMEM((T, 128), F32),
            pltpu.VMEM((TILES, 8, T), F32), pltpu.VMEM((TILES, 3, 8, T), F32),
            pltpu.VMEM((TILES, 8, T), F32), pltpu.VMEM((TILES, 3, 8, T), F32),
            pltpu.VMEM((3, TILES, T, 512), BF), pltpu.VMEM((TILES, T, 512), F32),
            tile, tile, tile,
            pltpu.VMEM((3, 32, 2, 32, 256), BF), pltpu.VMEM((3, 32, 32, 256), BF),
            pltpu.VMEM((3, 8, 4, 32, 256), BF), pltpu.VMEM((3, 3, 8, 32, 256), BF),
            pltpu.VMEM((3, 8, 32, 256), BF), pltpu.VMEM((3, 7, 32, 256), BF),
            pltpu.VMEM((3, 40, 256), F32), pltpu.VMEM((40, 256), F32),
            pltpu.VMEM((3, 40, 256), F32), pltpu.VMEM((7, 40, 256), F32),
            dma((2,)), dma((2,)),
            dma((TILES, 3)), dma((TILES, 3)), dma((TILES, 3)), dma((TILES, 3)),
            dma((TILES,)), dma((TILES,)), dma((TILES,)), dma((TILES,)), dma((TILES,)), dma((TILES,)),
            dma((3,)), dma((3,)), dma((3, 3)), dma((3, 3)), dma((3, 7)), dma((3, 7)),
            dma((11,)), dma((11,)),
        ],
        compiler_params=pltpu.CompilerParams(
            collective_id=0, has_side_effects=True, vmem_limit_bytes=62 * 1024 * 1024
        ),
        cost_estimate=pl.CostEstimate(
            flops=10_000_000_000, bytes_accessed=14_000_000, transcendentals=1_000_000
        ),
    )(x, g, wv, wg, taps, gain, shift, wp)


def placed(ig, w, sm, ig_out, v_out, g_out, p_out, t_out, gain_out, shift_out):
    ig_out[...] = ig[...]
    v_out[...] = w[1]
    g_out[...] = w[2]
    p_out[...] = w[0]
    t_out[...] = sm[0:TAPS]
    gain_out[...] = sm[TAPS : TAPS + 1]
    shift_out[...] = sm[TAPS + 1 : TAPS + 2]


def shards(block_input, out_grad, w_value, w_gate, conv_taps, norm_gain, norm_shift, w_proj):
    loss_scale = 1.0 / math.sqrt(block_input.shape[0] * lax.axis_size(SP))
    parts = module(
        loss_scale, block_input, out_grad, w_value, w_gate, conv_taps,
        norm_gain.reshape(1, -1), norm_shift.reshape(1, -1), w_proj,
    )
    shapes = [
        ((1024, 512), BF), ((32, 256), F32), ((32, 256), F32), ((32, 256), F32),
        ((TAPS, 256), F32), ((1, 256), F32), ((1, 256), F32),
    ]
    out = pl.pallas_call(
        placed,
        out_shape=tuple(jax.ShapeDtypeStruct(*shape) for shape in shapes),
        cost_estimate=pl.CostEstimate(flops=1_000_000, bytes_accessed=2_000_000, transcendentals=0),
    )(*parts)
    return (*out[:3], out[3].T, out[4], out[5].reshape(-1), out[6].reshape(-1))


def solution(mesh):
    return jax.shard_map(
        shards,
        mesh=mesh,
        in_specs=(
            P(SP, None),
            P(SP, None),
            P(None, "tp"),
            P(None, "tp"),
            P(None, "tp"),
            P("tp"),
            P("tp"),
            P("tp", None),
        ),
        out_specs=(
            P(SP, "tp"),
            P(SP, "tp"),
            P(SP, "tp"),
            P("tp", SP),
            P(None, "tp"),
            P("tp"),
            P("tp"),
        ),
        check_vma=False,
    )
```

```python
import functools
import math

import jax
import jax.numpy as jnp
from jax import lax
from jax.experimental import pallas as pl
from jax.experimental.pallas import tpu as pltpu
from jax.sharding import PartitionSpec as P

CH = 1024
SP = "sp"
MESH = pl.DeviceIdType.MESH
BF = jnp.bfloat16
F32 = jnp.float32
EPS = 0.05
TAPS = 31
T = 256
TILES = 4
R = 64


def plain(left, right):
    return jnp.dot(left, right, preferred_element_type=F32)


def rows_product(left, right):
    return lax.dot_general(left, right, (((1,), (1,)), ((), ())), preferred_element_type=F32)


def cols_product(left, right):
    return lax.dot_general(left, right, (((0,), (0,)), ((), ())), preferred_element_type=F32)


def logistic(v):
    return 0.5 * jnp.tanh(0.5 * v) + 0.5


def loop(count, body):
    def step(i, carry):
        body(i)
        return carry

    lax.fori_loop(0, count, step, 0)


def whole(
    scale,
    x_h, g_h, wv_h, wg_h, taps, gain, shift, wp_h,
    ig_out, w_out, sm_out,
    x, g, wv, wg, wp, load,
    gi, gi_halo, vf, sg, filt, gm, gf, gf_halo, gb, mx, tg, gs,
    sum_a, sum_b, col_m, col_i, col_a, col_b, st1, got1, st2, got2,
    part, own, got_a, got_b, got_c,
    wbuf, got_w, s1, got_y, s2, got_z,
    smb, sm_c, sm_y, sm_z,
    hs, hr, t1s, t1r, t2s, t2r, as_, ar, bs, br, cs, cr,
    ws, wr, ys, yr, zs, zr, ms, mr,
):
    s = lax.axis_index(SP)
    t = lax.axis_index("tp")
    c, y, z = s % 2, (s // 2) % 4, s // 8
    right, left, far = (t + 1) % 4, (t + 3) % 4, (t + 2) % 4
    last_sp = 63

    def local(src, dst, k):
        return pltpu.make_async_copy(src, dst, load.at[k])

    def x_rows(i):
        rows = pl.ds(i * T, T)
        return local(x_h.at[rows], x.at[rows], i)

    loads = [local(wv_h, wv, 4), local(wg_h, wg, 5)]
    loads[0].start()
    x_rows(3).start()
    loads[1].start()
    for i in range(3):
        x_rows(i).start()
    late = [local(wp_h, wp, 6), local(g_h, g, 7)]
    for copy in late:
        copy.start()

    def at_y(k):
        return {SP: (z * 4 + (y + k) % 4) * 2 + c}

    def at_z(k):
        return {SP: (((z + k) % 8) * 4 + y) * 2 + c}

    def at_t(k):
        return {"tp": (t + k) % 4}

    partner = {SP: s + 1 - 2 * c}
    after = {SP: (s + 1) % 64}
    before = {SP: (s + 63) % 64}
    peers = [at_t(k) for k in (1, 2, 3)] + [partner, after, before]
    peers += [at_y(k) for k in (1, 2, 3)] + [at_z(k) for k in range(1, 8)]
    barrier = pltpu.get_barrier_semaphore()
    for peer in peers:
        pl.semaphore_signal(barrier, inc=1, device_id=peer, device_id_type=MESH)

    def remote(src, dst, ssem, rsem, device):
        return pltpu.make_async_remote_copy(
            src_ref=src, dst_ref=dst, send_sem=ssem, recv_sem=rsem,
            device_id=device, device_id_type=MESH,
        )

    tg[...] = jnp.zeros_like(tg)
    gs[...] = jnp.zeros_like(gs)
    st1[...] = jnp.zeros_like(st1)
    st2[...] = jnp.zeros_like(st2)

    def token_sums(tile):
        return jnp.sum(tile[...].T, axis=0, keepdims=True)

    def over_lanes(row):
        return jnp.broadcast_to(row, (128, T)).T


    halo_send = remote(gi.at[:, pl.ds(1024, 32)], gi_halo, hs.at[0], hr.at[0], after)
    grad_send = remote(gf.at[:, pl.ds(0, 32)], gf_halo, hs.at[1], hr.at[1], before)

    def st1_send(i, k):
        return remote(st1.at[i], got1.at[i, k - 1], t1s.at[i, k - 1], t1r.at[i, k - 1], at_t(k))

    def st2_send(i, k):
        return remote(st2.at[i], got2.at[i, k - 1], t2s.at[i, k - 1], t2r.at[i, k - 1], at_t(k))

    def project(i):
        rows = pl.ds(pl.multiple_of(i * T, T), T)
        x_rows(i).wait()
        value = plain(x[rows, :], wv[...]).astype(BF).astype(F32)
        gate = plain(x[rows, :], wg[...]).astype(BF).astype(F32)
        sig = logistic(gate)
        gated = (value * sig).astype(BF).astype(F32)
        at = pl.ds(pl.multiple_of(i * T + 32, 32), T)
        for h in range(2):
            lanes = slice(h * 128, h * 128 + 128)
            vf[h, rows, :] = value[:, lanes]
            sg[h, rows, :] = sig[:, lanes]
            gi[h, at, :] = gated[:, lanes]

    def filter_tile(i):
        def block(b):
            base = pl.multiple_of(i * T + b * 128, 128)
            rows = pl.ds(base, 128)
            tile = pl.ds(pl.multiple_of(b * 128, 128), 128)
            for h in range(2):
                acc = jnp.zeros((128, 128), F32)
                for k in range(TAPS):
                    tap = taps[k : k + 1, h * 128 : h * 128 + 128]
                    acc = acc + tap * gi[h, pl.ds(base + 32 - k, 128), :]
                filt[h, rows, :] = acc
                if h == 0:
                    sum_a[tile, :] = acc
                    sum_b[tile, :] = acc * acc
                else:
                    sum_a[tile, :] = sum_a[tile, :] + acc
                    sum_b[tile, :] = sum_b[tile, :] + acc * acc

        loop(T // 128, block)
        st1[i, 0:1] = token_sums(sum_a)
        st1[i, 1:2] = token_sums(sum_b)
        for k in (1, 2, 3):
            st1_send(i, k).start()

    def mixed(i):
        rows = pl.ds(pl.multiple_of(i * T, T), T)
        out = rows_product(g[rows, :], wp[...])
        for h in range(2):
            gm[h, rows, :] = out[:, h * 128 : h * 128 + 128]

    def activate(i):
        for k in (1, 2, 3):
            st1_send(i, k).wait_recv()
        sums = st1[i] + got1[i, 0] + got1[i, 1] + got1[i, 2]
        mean = sums[0:1] / CH
        var = sums[1:2] / CH - mean * mean
        col_m[i] = over_lanes(mean)
        col_i[i] = over_lanes(lax.rsqrt(var + EPS))

        def block(b):
            local_rows = pl.ds(pl.multiple_of(b * R, R), R)
            rows = pl.ds(pl.multiple_of(i * T + b * R, R), R)
            mean = col_m[i, local_rows, :]
            inv = col_i[i, local_rows, :]
            first, second = 0.0, 0.0
            for h in range(2):
                lanes = slice(h * 128, h * 128 + 128)
                normed = (filt[h, rows, :] - mean) * inv
                act = normed * gain[0:1, lanes] + shift[0:1, lanes]
                sig = logistic(act)
                mx[rows, lanes] = (act * sig).astype(BF)
                grad = gm[h, rows, :] * sig * (1.0 + act * (1.0 - sig))
                gs[0, h] = gs[0, h] + (grad * normed).reshape(R // 8, 8, 128).sum(axis=0)
                gs[1, h] = gs[1, h] + grad.reshape(R // 8, 8, 128).sum(axis=0)
                grad = grad * gain[0:1, lanes]
                filt[h, rows, :] = normed
                gm[h, rows, :] = grad
                first = first + grad
                second = second + grad * normed
            sum_a[local_rows, :] = first
            sum_b[local_rows, :] = second

        loop(T // R, block)
        st2[i, 0:1] = token_sums(sum_a)
        st2[i, 1:2] = token_sums(sum_b)
        for k in (1, 2, 3):
            st2_send(i, k).start()

    def pair_send(n, q):
        rows = pl.ds(q * 8, 8)
        return remote(
            wbuf.at[n, rows, 1 - c], got_w.at[n, rows], ws.at[n, q], wr.at[n, q], partner
        )

    def y_way(q):
        return jnp.where(q == 0, (y + 1) % 4, (y + 3) % 4), jnp.where(q == 0, (y + 3) % 4, (y + 1) % 4)

    def y_move(kind, n, q, which, line):
        rows = pl.ds(q * 4, 4)
        return remote(
            s1.at[n, rows, which], got_y.at[kind, n, rows], ys.at[kind, n, q], yr.at[kind, n, q],
            {SP: (z * 4 + line) * 2 + c},
        )

    def ya_send(n, q):
        return y_move(0, n, q, (y + 2) % 4, y_way(q)[0])

    def yb_send(n, q):
        return y_move(1, n, q, y_way(q)[1], y_way(q)[1])

    def yc_send(n, q):
        return y_move(2, n, q, y_way(q)[0], y_way(q)[0])

    def z_send(n, k):
        return remote(
            s2.at[n, (z + k) % 8], got_z.at[n, k - 1], zs.at[n, k - 1], zr.at[n, k - 1], at_z(k)
        )

    def proj_half(first):
        def tile(j):
            zb = first + j
            span = pl.ds(pl.multiple_of(zb * 512, 512), 512)
            out = cols_product(g[:, span], mx[...]).astype(BF)
            wbuf[0, pl.ds(zb * 8, 8)] = out.reshape(8, 2, 32, 256)
            pair_send(0, zb).start()

        loop(2, tile)

    def gate_chunks():
        def tile(zb):
            span = pl.ds(pl.multiple_of(zb * 512, 512), 512)
            out = cols_product(x[:, span], gb[...]).astype(BF)
            for n in (0, 1):
                wbuf[n + 1, pl.ds(zb * 8, 8)] = out[:, n * 256 : n * 256 + 256].reshape(8, 2, 32, 256)
                pair_send(n + 1, zb).start()

        loop(4, tile)

    def pair_sum(n):
        def tile(q):
            pair_send(n, q).wait_recv()
            for r in range(2):
                rows = pl.ds(q * 8 + r * 4, 4)
                pair = wbuf[n, rows, c].astype(F32) + got_w[n, rows].astype(F32)
                s1[n, q * 2 + r] = pair.astype(BF)

        loop(4, tile)
        for q in (0, 1):
            ya_send(n, q).start()
        for q in (0, 1):
            yb_send(n, q).start()

    def y_pass(n):
        for q in (0, 1):
            ya_send(n, q).wait_recv()
            rows, line = pl.ds(q * 4, 4), y_way(q)[0]
            pair = s1[n, rows, line].astype(F32) + got_y[0, n, rows].astype(F32)
            s1[n, rows, line] = pair.astype(BF)
            yc_send(n, q).start()

    def y_sum(n):
        for q in (0, 1):
            yb_send(n, q).wait_recv()
            yc_send(n, q).wait_recv()
        total = s1[n, :, y].astype(F32) + got_y[1, n].astype(F32) + got_y[2, n].astype(F32)
        s2[n] = total.astype(BF)
        for k in range(1, 8):
            z_send(n, k).start()

    def z_sum(n):
        for k in range(1, 8):
            z_send(n, k).wait_recv()
        total = s2[n, z].astype(F32)
        for k in range(7):
            total = total + got_z[n, k].astype(F32)
        w_out[n] = total * scale

    def filtered_grad(i):
        for k in (1, 2, 3):
            st2_send(i, k).wait_recv()
        sums = (st2[i] + got2[i, 0] + got2[i, 1] + got2[i, 2]) / CH
        col_a[...] = over_lanes(sums[0:1])
        col_b[...] = over_lanes(sums[1:2])

        def block(b):
            local_rows = pl.ds(pl.multiple_of(b * R, R), R)
            rows = pl.ds(pl.multiple_of(i * T + b * R, R), R)
            inv = col_i[i, local_rows, :]
            m1 = col_a[local_rows, :]
            m2 = col_b[local_rows, :]
            for h in range(2):
                gf[h, rows, :] = inv * (gm[h, rows, :] - m1 - filt[h, rows, :] * m2)

        loop(T // R, block)

    def toward(i):
        first = i < TILES // 2
        return jnp.where(first, right, left), jnp.where(first, left, right)

    def a_send(i):
        return remote(part.at[0, i], got_a.at[i], as_.at[i], ar.at[i], {"tp": toward(i)[0]})

    def b_send(i):
        return remote(part.at[1, i], got_b.at[i], bs.at[i], br.at[i], {"tp": toward(i)[1]})

    def c_send(i):
        return remote(part.at[2, i], got_c.at[i], cs.at[i], cr.at[i], {"tp": toward(i)[0]})

    def back_tile(i):
        for h in range(2):
            lanes = slice(h * 128, h * 128 + 128)
            lanes_g = slice(256 + h * 128, 384 + h * 128)

            def block(b, h=h, lanes=lanes, lanes_g=lanes_g):
                base = pl.multiple_of(i * T + b * R, R)
                rows = pl.ds(base, R)
                gated = gi[h, pl.ds(pl.multiple_of(base + 32, 32), R), :]
                acc = jnp.zeros((R, 128), F32)
                for k in range(TAPS):
                    moved = gf[h, pl.ds(base + k, R), :]
                    acc = acc + taps[k : k + 1, lanes] * moved
                    tg[h, k] = tg[h, k] + (gated * moved).reshape(R // 8, 8, 128).sum(axis=0)
                sig = sg[h, rows, :]
                gv = acc * sig
                gb[rows, lanes] = gv.astype(BF)
                gb[rows, lanes_g] = (gv * vf[h, rows, :] * (1.0 - sig)).astype(BF)

            loop(T // R, block)

        rows = pl.ds(pl.multiple_of(i * T, T), T)

        def partial(block):
            span = pl.ds(pl.multiple_of(block * 512, 512), 512)
            return rows_product(gb[rows, 0:256], wv[span, :]) + rows_product(
                gb[rows, 256:512], wg[span, :]
            )

        near, back = toward(i)
        part[0, i] = partial(far).astype(BF)
        a_send(i).start()
        part[1, i] = partial(back).astype(BF)
        b_send(i).start()
        part[2, i] = partial(near).astype(BF)
        own[i] = partial(t)

    def combine(i):
        a_send(i).wait_recv()
        part[2, i] = (part[2, i].astype(F32) + got_a[i].astype(F32)).astype(BF)
        c_send(i).start()

    def pair(first, body):
        loop(2, lambda j: body(first + j))

    for copy in loads:
        copy.wait()
    project(3)
    pl.semaphore_wait(barrier, len(peers))
    halo_send.start()
    loop(3, project)
    for copy in late:
        copy.wait()
    pair(0, mixed)
    halo_send.wait_recv()
    gi[:, 0:32, :] = jnp.where(s == 0, 0.0, gi_halo[...])
    loop(TILES, filter_tile)
    pair(2, mixed)
    loop(TILES, activate)
    proj_half(0)
    filtered_grad(0)
    grad_send.start()

    def middle(j):
        @pl.when(j < 3)
        def _():
            filtered_grad(j + 1)

        @pl.when(j == 1)
        def _():
            proj_half(2)

        @pl.when(j == 2)
        def _():
            pair_sum(0)

        @pl.when(j == 3)
        def _():
            grad_send.wait_recv()
            gf[:, 1024:1056, :] = jnp.where(s == last_sp, 0.0, gf_halo[...])

        back_tile(j)

    loop(TILES, middle)

    for h in range(2):
        smb[h, 0:TAPS] = jnp.sum(tg[h], axis=1)
        smb[h, 31:32] = jnp.sum(gs[0, h], axis=0, keepdims=True)
        smb[h, 32:33] = jnp.sum(gs[1, h], axis=0, keepdims=True)
        smb[h, 33:40] = jnp.zeros((7, 128), F32)
    sm_pair = remote(smb.at[1 - c], sm_c, ms.at[0], mr.at[0], partner)
    sm_pair.start()
    y_pass(0)
    gate_chunks()
    sm_pair.wait_recv()
    smb[2] = smb[c] + sm_c[...]
    sm_ys = [remote(smb.at[2], sm_y.at[k - 1], ms.at[k], mr.at[k], at_y(k)) for k in (1, 2, 3)]
    for copy in sm_ys:
        copy.start()
    loop(2, lambda j: pair_sum(j + 1))
    y_sum(0)
    combine(0)
    for copy in sm_ys:
        copy.wait_recv()
    smb[3] = smb[2] + sm_y[0] + sm_y[1] + sm_y[2]
    sm_zs = [
        remote(smb.at[3], sm_z.at[k - 1], ms.at[3 + k], mr.at[3 + k], at_z(k)) for k in range(1, 8)
    ]
    for copy in sm_zs:
        copy.start()
    y_pass(1)
    combine(1)
    y_pass(2)
    combine(2)
    y_sum(1)
    y_sum(2)
    combine(3)
    for copy in sm_zs:
        copy.wait_recv()
    total = smb[3]
    for k in range(7):
        total = total + sm_z[k]
    smb[4] = total * scale
    sm_swap = remote(smb.at[4], smb.at[5], ms.at[11], mr.at[11], partner)
    sm_swap.start()
    z_sum(0)
    sm_swap.wait_recv()
    sm_out[c] = smb[4]
    sm_out[1 - c] = smb[5]
    loop(2, lambda j: z_sum(j + 1))

    def finish(i):
        b_send(i).wait_recv()
        c_send(i).wait_recv()
        rows = pl.ds(i * T, T)
        ig_out[rows, :] = (own[i] + got_b[i].astype(F32) + got_c[i].astype(F32)).astype(BF)

    for i in (0, 2, 1, 3):
        finish(i)

    halo_send.wait_send()
    grad_send.wait_send()
    for copy in [sm_pair, sm_swap, *sm_ys, *sm_zs]:
        copy.wait_send()
    for n in range(3):
        for q in range(4):
            pair_send(n, q).wait_send()
        for q in (0, 1):
            ya_send(n, q).wait_send()
            yb_send(n, q).wait_send()
            yc_send(n, q).wait_send()
        for k in range(1, 8):
            z_send(n, k).wait_send()

    def drain(i):
        for k in (1, 2, 3):
            st1_send(i, k).wait_send()
            st2_send(i, k).wait_send()
        a_send(i).wait_send()
        b_send(i).wait_send()
        c_send(i).wait_send()

    loop(TILES, drain)


def module(scale, x, g, wv, wg, taps, gain, shift, wp):
    dma = pltpu.SemaphoreType.DMA
    vmem = pl.BlockSpec(memory_space=pltpu.VMEM)
    hbm = pl.BlockSpec(memory_space=pl.ANY)

    def half(rows, kind=F32):
        return pltpu.VMEM((2, rows, 128), kind)

    tile = pltpu.VMEM((TILES, T, 512), BF)
    return pl.pallas_call(
        functools.partial(whole, scale),
        out_shape=(
            jax.ShapeDtypeStruct((1024, 512), BF),
            jax.ShapeDtypeStruct((3, 32, 256), F32),
            jax.ShapeDtypeStruct((2, 40, 128), F32),
        ),
        in_specs=[hbm, hbm, hbm, hbm, vmem, vmem, vmem, hbm],
        out_specs=(vmem,) * 3,
        scratch_shapes=[
            pltpu.VMEM((1024, 2048), BF), pltpu.VMEM((1024, 2048), BF),
            pltpu.VMEM((2048, 256), BF), pltpu.VMEM((2048, 256), BF), pltpu.VMEM((256, 2048), BF),
            dma((8,)),
            half(1056), half(32), half(1024), half(1024), half(1024), half(1024), half(1056), half(32),
            pltpu.VMEM((1024, 512), BF), pltpu.VMEM((1024, 256), BF),
            pltpu.VMEM((2, TAPS, 8, 128), F32), pltpu.VMEM((2, 2, 8, 128), F32),
            pltpu.VMEM((T, 128), F32), pltpu.VMEM((T, 128), F32),
            pltpu.VMEM((TILES, T, 128), F32), pltpu.VMEM((TILES, T, 128), F32),
            pltpu.VMEM((T, 128), F32), pltpu.VMEM((T, 128), F32),
            pltpu.VMEM((TILES, 8, T), F32), pltpu.VMEM((TILES, 3, 8, T), F32),
            pltpu.VMEM((TILES, 8, T), F32), pltpu.VMEM((TILES, 3, 8, T), F32),
            pltpu.VMEM((3, TILES, T, 512), BF), pltpu.VMEM((TILES, T, 512), F32),
            tile, tile, tile,
            pltpu.VMEM((3, 32, 2, 32, 256), BF), pltpu.VMEM((3, 32, 32, 256), BF),
            pltpu.VMEM((3, 8, 4, 32, 256), BF), pltpu.VMEM((3, 3, 8, 32, 256), BF),
            pltpu.VMEM((3, 8, 32, 256), BF), pltpu.VMEM((3, 7, 32, 256), BF),
            pltpu.VMEM((6, 40, 128), F32), pltpu.VMEM((40, 128), F32),
            pltpu.VMEM((3, 40, 128), F32), pltpu.VMEM((7, 40, 128), F32),
            dma((2,)), dma((2,)),
            dma((TILES, 3)), dma((TILES, 3)), dma((TILES, 3)), dma((TILES, 3)),
            dma((TILES,)), dma((TILES,)), dma((TILES,)), dma((TILES,)), dma((TILES,)), dma((TILES,)),
            dma((3, 4)), dma((3, 4)), dma((3, 3, 2)), dma((3, 3, 2)), dma((3, 7)), dma((3, 7)),
            dma((12,)), dma((12,)),
        ],
        compiler_params=pltpu.CompilerParams(
            collective_id=0, has_side_effects=True, vmem_limit_bytes=62 * 1024 * 1024
        ),
        cost_estimate=pl.CostEstimate(
            flops=10_000_000_000, bytes_accessed=14_000_000, transcendentals=1_000_000
        ),
    )(x, g, wv, wg, taps, gain, shift, wp)


def placed(ig, w, sm, ig_out, v_out, g_out, p_out, t_out, gain_out, shift_out):
    ig_out[...] = ig[...]

    @pl.when(pl.program_id(0) == 0)
    def _():
        v_out[...] = w[1]
        g_out[...] = w[2]
        p_out[...] = w[0]
        for h in range(2):
            lanes = slice(h * 128, h * 128 + 128)
            t_out[:, lanes] = sm[h, 0:TAPS]
            gain_out[:, lanes] = sm[h, TAPS : TAPS + 1]
            shift_out[:, lanes] = sm[h, TAPS + 1 : TAPS + 2]


def fixed(*shape):
    return pl.BlockSpec(shape, lambda i: (0,) * len(shape))


def shards(block_input, out_grad, w_value, w_gate, conv_taps, norm_gain, norm_shift, w_proj):
    loss_scale = 1.0 / math.sqrt(block_input.shape[0] * lax.axis_size(SP))
    parts = module(
        loss_scale, block_input, out_grad, w_value, w_gate, conv_taps,
        norm_gain.reshape(1, -1), norm_shift.reshape(1, -1), w_proj,
    )
    shapes = [
        ((1024, 512), BF), ((32, 256), F32), ((32, 256), F32), ((32, 256), F32),
        ((TAPS, 256), F32), ((1, 256), F32), ((1, 256), F32),
    ]
    out = pl.pallas_call(
        placed,
        grid=(2,),
        in_specs=[pl.BlockSpec((512, 512), lambda i: (i, 0)), fixed(3, 32, 256), fixed(2, 40, 128)],
        out_specs=[pl.BlockSpec((512, 512), lambda i: (i, 0))]
        + [fixed(*shape) for shape, _ in shapes[1:]],
        out_shape=[jax.ShapeDtypeStruct(*shape) for shape in shapes],
        cost_estimate=pl.CostEstimate(flops=1_000_000, bytes_accessed=2_000_000, transcendentals=0),
    )(*parts)
    return (*out[:3], out[3].T, out[4], out[5].reshape(-1), out[6].reshape(-1))


def solution(mesh):
    return jax.shard_map(
        shards,
        mesh=mesh,
        in_specs=(
            P(SP, None),
            P(SP, None),
            P(None, "tp"),
            P(None, "tp"),
            P(None, "tp"),
            P("tp"),
            P("tp"),
            P("tp", None),
        ),
        out_specs=(
            P(SP, "tp"),
            P(SP, "tp"),
            P(SP, "tp"),
            P("tp", SP),
            P(None, "tp"),
            P("tp"),
            P("tp"),
        ),
        check_vma=False,
    )
```

```python
import functools
import math

import jax
import jax.numpy as jnp
from jax import lax
from jax.experimental import pallas as pl
from jax.experimental.pallas import tpu as pltpu
from jax.sharding import PartitionSpec as P

CH = 1024
SP = "sp"
MESH = pl.DeviceIdType.MESH
BF = jnp.bfloat16
F32 = jnp.float32
EPS = 0.05
TAPS = 31
T = 256
TILES = 4
R = 64


def plain(left, right):
    return jnp.dot(left, right, preferred_element_type=F32)


def rows_product(left, right):
    return lax.dot_general(left, right, (((1,), (1,)), ((), ())), preferred_element_type=F32)


def cols_product(left, right):
    return lax.dot_general(left, right, (((0,), (0,)), ((), ())), preferred_element_type=F32)


def logistic(v):
    return 0.5 * jnp.tanh(0.5 * v) + 0.5


def loop(count, body):
    def step(i, carry):
        body(i)
        return carry

    lax.fori_loop(0, count, step, 0)


def whole(
    scale,
    x_h, g_h, wv_h, wg_h, taps, gain, shift, wp_h,
    ig_out, w_out, sm_out,
    x, g, wv, wg, wp, load,
    gi, gi_halo, vf, sg, filt, gm, gf, gf_halo, gb, mx, tg, gs,
    sum_a, sum_b, col_m, col_i, col_a, col_b, st1, got1, st2, got2,
    part, own, got_a, got_b, got_c,
    wbuf, got_w, s1, got_y, s2, got_z,
    smb, sm_c, sm_y, sm_z,
    hs, hr, t1s, t1r, t2s, t2r, as_, ar, bs, br, cs, cr,
    ws, wr, ys, yr, zs, zr, ms, mr,
):
    s = lax.axis_index(SP)
    t = lax.axis_index("tp")
    c, y, z = s % 2, (s // 2) % 4, s // 8
    right, left, far = (t + 1) % 4, (t + 3) % 4, (t + 2) % 4
    last_sp = 63

    def local(src, dst, k):
        return pltpu.make_async_copy(src, dst, load.at[k])

    def x_rows(i):
        rows = pl.ds(i * T, T)
        return local(x_h.at[rows], x.at[rows], i)

    loads = [local(wv_h, wv, 4), local(wg_h, wg, 5)]
    loads[0].start()
    x_rows(3).start()
    loads[1].start()
    for i in range(3):
        x_rows(i).start()
    late = [local(wp_h, wp, 6), local(g_h, g, 7)]
    for copy in late:
        copy.start()

    def at_y(k):
        return {SP: (z * 4 + (y + k) % 4) * 2 + c}

    def at_z(k):
        return {SP: (((z + k) % 8) * 4 + y) * 2 + c}

    def at_t(k):
        return {"tp": (t + k) % 4}

    partner = {SP: s + 1 - 2 * c}
    after = {SP: (s + 1) % 64}
    before = {SP: (s + 63) % 64}
    peers = [at_t(k) for k in (1, 2, 3)] + [partner, after, before]
    peers += [at_y(k) for k in (1, 2, 3)] + [at_z(k) for k in range(1, 8)]
    barrier = pltpu.get_barrier_semaphore()
    for peer in peers:
        pl.semaphore_signal(barrier, inc=1, device_id=peer, device_id_type=MESH)

    def remote(src, dst, ssem, rsem, device):
        return pltpu.make_async_remote_copy(
            src_ref=src, dst_ref=dst, send_sem=ssem, recv_sem=rsem,
            device_id=device, device_id_type=MESH,
        )

    tg[...] = jnp.zeros_like(tg)
    gs[...] = jnp.zeros_like(gs)
    st1[...] = jnp.zeros_like(st1)
    st2[...] = jnp.zeros_like(st2)

    def token_sums(tile):
        return jnp.sum(tile[...].T, axis=0, keepdims=True)

    def over_lanes(row):
        return jnp.broadcast_to(row, (128, T)).T


    halo_send = remote(gi.at[:, pl.ds(1024, 32)], gi_halo, hs.at[0], hr.at[0], after)
    grad_send = remote(gf.at[:, pl.ds(0, 32)], gf_halo, hs.at[1], hr.at[1], before)

    def st1_send(i, k):
        return remote(st1.at[i], got1.at[i, k - 1], t1s.at[i, k - 1], t1r.at[i, k - 1], at_t(k))

    def st2_send(i, k):
        return remote(st2.at[i], got2.at[i, k - 1], t2s.at[i, k - 1], t2r.at[i, k - 1], at_t(k))

    def project(i):
        rows = pl.ds(pl.multiple_of(i * T, T), T)
        x_rows(i).wait()
        value = plain(x[rows, :], wv[...]).astype(BF).astype(F32)
        gate = plain(x[rows, :], wg[...]).astype(BF).astype(F32)
        sig = logistic(gate)
        gated = (value * sig).astype(BF).astype(F32)
        at = pl.ds(pl.multiple_of(i * T + 32, 32), T)
        for h in range(2):
            lanes = slice(h * 128, h * 128 + 128)
            vf[h, rows, :] = value[:, lanes]
            sg[h, rows, :] = sig[:, lanes]
            gi[h, at, :] = gated[:, lanes]

    def filter_rows(i):
        def block(b):
            base = pl.multiple_of(i * T + b * 128, 128)
            rows = pl.ds(base, 128)
            tile = pl.ds(pl.multiple_of(b * 128, 128), 128)
            for h in range(2):
                acc = jnp.zeros((128, 128), F32)
                for k in range(TAPS):
                    tap = taps[k : k + 1, h * 128 : h * 128 + 128]
                    acc = acc + tap * gi[h, pl.ds(base + 32 - k, 128), :]
                filt[h, rows, :] = acc
                if h == 0:
                    sum_a[tile, :] = acc
                    sum_b[tile, :] = acc * acc
                else:
                    sum_a[tile, :] = sum_a[tile, :] + acc
                    sum_b[tile, :] = sum_b[tile, :] + acc * acc

        loop(T // 128, block)
        st1[i, 0:1] = token_sums(sum_a)
        st1[i, 1:2] = token_sums(sum_b)

    def filter_tell(i):
        for k in (2, 1, 3):
            st1_send(i, k).start()

    def filter_tile(i):
        filter_rows(i)
        filter_tell(i)

    def mixed(i):
        rows = pl.ds(pl.multiple_of(i * T, T), T)
        out = rows_product(g[rows, :], wp[...])
        for h in range(2):
            gm[h, rows, :] = out[:, h * 128 : h * 128 + 128]

    def activate(i):
        for k in (1, 2, 3):
            st1_send(i, k).wait_recv()
        sums = st1[i] + got1[i, 0] + got1[i, 1] + got1[i, 2]
        mean = sums[0:1] / CH
        var = sums[1:2] / CH - mean * mean
        col_m[i] = over_lanes(mean)
        col_i[i] = over_lanes(lax.rsqrt(var + EPS))

        def block(b):
            local_rows = pl.ds(pl.multiple_of(b * R, R), R)
            rows = pl.ds(pl.multiple_of(i * T + b * R, R), R)
            mean = col_m[i, local_rows, :]
            inv = col_i[i, local_rows, :]
            first, second = 0.0, 0.0
            for h in range(2):
                lanes = slice(h * 128, h * 128 + 128)
                normed = (filt[h, rows, :] - mean) * inv
                act = normed * gain[0:1, lanes] + shift[0:1, lanes]
                sig = logistic(act)
                mx[rows, lanes] = (act * sig).astype(BF)
                grad = gm[h, rows, :] * sig * (1.0 + act * (1.0 - sig))
                gs[0, h] = gs[0, h] + (grad * normed).reshape(R // 8, 8, 128).sum(axis=0)
                gs[1, h] = gs[1, h] + grad.reshape(R // 8, 8, 128).sum(axis=0)
                grad = grad * gain[0:1, lanes]
                filt[h, rows, :] = normed
                gm[h, rows, :] = grad
                first = first + grad
                second = second + grad * normed
            sum_a[local_rows, :] = first
            sum_b[local_rows, :] = second

        loop(T // R, block)
        st2[i, 0:1] = token_sums(sum_a)
        st2[i, 1:2] = token_sums(sum_b)
        for k in (1, 2, 3):
            st2_send(i, k).start()

    def pair_send(n, q):
        rows = pl.ds(q * 8, 8)
        return remote(
            wbuf.at[n, rows, 1 - c], got_w.at[n, rows], ws.at[n, q], wr.at[n, q], partner
        )

    def y_way(q):
        return jnp.where(q == 0, (y + 1) % 4, (y + 3) % 4), jnp.where(q == 0, (y + 3) % 4, (y + 1) % 4)

    def y_move(kind, n, q, which, line):
        rows = pl.ds(q * 4, 4)
        return remote(
            s1.at[n, rows, which], got_y.at[kind, n, rows], ys.at[kind, n, q], yr.at[kind, n, q],
            {SP: (z * 4 + line) * 2 + c},
        )

    def ya_send(n, q):
        return y_move(0, n, q, (y + 2) % 4, y_way(q)[0])

    def yb_send(n, q):
        return y_move(1, n, q, y_way(q)[1], y_way(q)[1])

    def yc_send(n, q):
        return y_move(2, n, q, y_way(q)[0], y_way(q)[0])

    def z_send(n, k):
        return remote(
            s2.at[n, (z + k) % 8], got_z.at[n, k - 1], zs.at[n, k - 1], zr.at[n, k - 1], at_z(k)
        )

    def proj_half(first):
        def tile(j):
            zb = first + j
            span = pl.ds(pl.multiple_of(zb * 512, 512), 512)
            out = cols_product(g[:, span], mx[...]).astype(BF)
            wbuf[0, pl.ds(zb * 8, 8)] = out.reshape(8, 2, 32, 256)
            pair_send(0, zb).start()

        loop(2, tile)

    def gate_chunks(first, count):
        def tile(j):
            zb = first + j
            span = pl.ds(pl.multiple_of(zb * 512, 512), 512)
            out = cols_product(x[:, span], gb[...]).astype(BF)
            for n in (0, 1):
                wbuf[n + 1, pl.ds(zb * 8, 8)] = out[:, n * 256 : n * 256 + 256].reshape(8, 2, 32, 256)
                pair_send(n + 1, zb).start()

        loop(count, tile)

    def pair_half(n, q):
        def tile(j):
            pair_send(n, q * 2 + j).wait_recv()
            for r in range(2):
                rows = pl.ds(q * 8 * 2 + j * 8 + r * 4, 4)
                s1[n, q * 4 + j * 2 + r] = wbuf[n, rows, c] + got_w[n, rows]

        loop(2, tile)
        ya_send(n, q).start()
        yb_send(n, q).start()

    def pair_sum(n):
        pair_half(n, 0)
        pair_half(n, 1)

    def y_pass(n):
        for q in (0, 1):
            ya_send(n, q).wait_recv()
            rows, line = pl.ds(q * 4, 4), y_way(q)[0]
            s1[n, rows, line] = s1[n, rows, line] + got_y[0, n, rows]
            yc_send(n, q).start()

    def y_sum(n):
        for q in (0, 1):
            yb_send(n, q).wait_recv()
            yc_send(n, q).wait_recv()
        total = s1[n, :, y].astype(F32) + got_y[1, n].astype(F32) + got_y[2, n].astype(F32)
        s2[n] = total.astype(BF)
        for k in range(1, 8):
            z_send(n, k).start()

    def z_sum(n):
        for k in range(1, 8):
            z_send(n, k).wait_recv()
        total = s2[n, z].astype(F32)
        for k in range(7):
            total = total + got_z[n, k].astype(F32)
        w_out[n] = total * scale

    def filtered_grad(i):
        for k in (1, 2, 3):
            st2_send(i, k).wait_recv()
        sums = (st2[i] + got2[i, 0] + got2[i, 1] + got2[i, 2]) / CH
        col_a[...] = over_lanes(sums[0:1])
        col_b[...] = over_lanes(sums[1:2])

        def block(b):
            local_rows = pl.ds(pl.multiple_of(b * R, R), R)
            rows = pl.ds(pl.multiple_of(i * T + b * R, R), R)
            inv = col_i[i, local_rows, :]
            m1 = col_a[local_rows, :]
            m2 = col_b[local_rows, :]
            for h in range(2):
                gf[h, rows, :] = inv * (gm[h, rows, :] - m1 - filt[h, rows, :] * m2)

        loop(T // R, block)

    def toward(i):
        first = i < TILES // 2
        return jnp.where(first, right, left), jnp.where(first, left, right)

    def a_send(i):
        return remote(part.at[0, i], got_a.at[i], as_.at[i], ar.at[i], {"tp": toward(i)[0]})

    def b_send(i):
        return remote(part.at[1, i], got_b.at[i], bs.at[i], br.at[i], {"tp": toward(i)[1]})

    def c_send(i):
        return remote(part.at[2, i], got_c.at[i], cs.at[i], cr.at[i], {"tp": toward(i)[0]})

    def partial(i, block):
        rows = pl.ds(pl.multiple_of(i * T, T), T)
        span = pl.ds(pl.multiple_of(block * 512, 512), 512)
        return rows_product(gb[rows, 0:256], wv[span, :]) + rows_product(
            gb[rows, 256:512], wg[span, :]
        )

    def back_tile(i):
        for h in range(2):
            lanes = slice(h * 128, h * 128 + 128)
            lanes_g = slice(256 + h * 128, 384 + h * 128)

            def block(b, h=h, lanes=lanes, lanes_g=lanes_g):
                base = pl.multiple_of(i * T + b * R, R)
                rows = pl.ds(base, R)
                gated = gi[h, pl.ds(pl.multiple_of(base + 32, 32), R), :]
                acc = jnp.zeros((R, 128), F32)
                for k in range(TAPS):
                    moved = gf[h, pl.ds(base + k, R), :]
                    acc = acc + taps[k : k + 1, lanes] * moved
                    tg[h, k] = tg[h, k] + (gated * moved).reshape(R // 8, 8, 128).sum(axis=0)
                sig = sg[h, rows, :]
                gv = acc * sig
                gb[rows, lanes] = gv.astype(BF)
                gb[rows, lanes_g] = (gv * vf[h, rows, :] * (1.0 - sig)).astype(BF)

            loop(T // R, block)

        part[0, i] = partial(i, far).astype(BF)
        a_send(i).start()
        part[1, i] = partial(i, toward(i)[1]).astype(BF)
        b_send(i).start()

    def near_tile(i):
        part[2, i] = partial(i, toward(i)[0]).astype(BF)
        own[i] = partial(i, t)

    def combine(i):
        a_send(i).wait_recv()
        part[2, i] = part[2, i] + got_a[i]
        c_send(i).start()

    def gather(i):
        b_send(i).wait_recv()
        own[i] = own[i] + got_b[i].astype(F32)

    def pair(first, body):
        loop(2, lambda j: body(first + j))

    for copy in loads:
        copy.wait()
    loop(TILES, lambda j: project((j + 3) % 4))
    filter_rows(1)
    pl.semaphore_wait(barrier, len(peers))
    halo_send.start()
    filter_tell(1)
    pair(2, filter_tile)
    for copy in late:
        copy.wait()
    pair(1, mixed)
    halo_send.wait_recv()
    gi[:, 0:32, :] = jnp.where(s == 0, 0.0, gi_halo[...])
    filter_tile(0)
    pair(1, activate)
    loop(2, lambda j: mixed((j + 3) % 4))
    loop(2, lambda j: activate((j + 3) % 4))
    proj_half(0)
    pair(1, filtered_grad)

    def middle(j):
        @pl.when(j == 1)
        def _():
            proj_half(2)
            filtered_grad(3)
            filtered_grad(0)
            grad_send.start()

        @pl.when(j == 3)
        def _():
            pair_sum(0)
            grad_send.wait_recv()
            gf[:, 1024:1056, :] = jnp.where(s == last_sp, 0.0, gf_halo[...])

        back_tile(jnp.where(j == 3, 3, (j + 1) % 3))

    loop(TILES, middle)

    for h in range(2):
        smb[h, 0:TAPS] = jnp.sum(tg[h], axis=1)
        smb[h, 31:32] = jnp.sum(gs[0, h], axis=0, keepdims=True)
        smb[h, 32:33] = jnp.sum(gs[1, h], axis=0, keepdims=True)
        smb[h, 33:40] = jnp.zeros((7, 128), F32)
    sm_pair = remote(smb.at[1 - c], sm_c, ms.at[0], mr.at[0], partner)
    sm_pair.start()
    y_pass(0)
    gate_chunks(0, 3)
    loop(2, lambda j: pair_half(j + 1, 0))
    gate_chunks(3, 1)
    loop(TILES, near_tile)
    sm_pair.wait_recv()
    smb[2] = smb[c] + sm_c[...]
    sm_ys = [remote(smb.at[2], sm_y.at[k - 1], ms.at[k], mr.at[k], at_y(k)) for k in (1, 2, 3)]
    for copy in sm_ys:
        copy.start()
    loop(2, lambda j: pair_half(j + 1, 1))
    y_sum(0)
    combine(1)
    for copy in sm_ys:
        copy.wait_recv()
    smb[3] = smb[2] + sm_y[0] + sm_y[1] + sm_y[2]
    sm_zs = [
        remote(smb.at[3], sm_z.at[k - 1], ms.at[3 + k], mr.at[3 + k], at_z(k)) for k in range(1, 8)
    ]
    for copy in sm_zs:
        copy.start()
    y_pass(1)
    combine(2)
    y_pass(2)
    combine(0)
    y_sum(1)
    y_sum(2)
    combine(3)
    for copy in sm_zs:
        copy.wait_recv()
    total = smb[3]
    for k in range(7):
        total = total + sm_z[k]
    smb[4] = total * scale
    sm_swap = remote(smb.at[4], smb.at[5], ms.at[11], mr.at[11], partner)
    sm_swap.start()
    loop(TILES, gather)
    z_sum(0)
    sm_swap.wait_recv()
    sm_out[c] = smb[4]
    sm_out[1 - c] = smb[5]
    loop(2, lambda j: z_sum(j + 1))

    def finish(i):
        c_send(i).wait_recv()
        rows = pl.ds(i * T, T)
        ig_out[rows, :] = (own[i] + got_c[i].astype(F32)).astype(BF)

    for i in (1, 2, 0, 3):
        finish(i)

    halo_send.wait_send()
    grad_send.wait_send()
    for copy in [sm_pair, sm_swap, *sm_ys, *sm_zs]:
        copy.wait_send()
    for n in range(3):
        for q in range(4):
            pair_send(n, q).wait_send()
        for q in (0, 1):
            ya_send(n, q).wait_send()
            yb_send(n, q).wait_send()
            yc_send(n, q).wait_send()
        for k in range(1, 8):
            z_send(n, k).wait_send()

    def drain(i):
        for k in (1, 2, 3):
            st1_send(i, k).wait_send()
            st2_send(i, k).wait_send()
        a_send(i).wait_send()
        b_send(i).wait_send()
        c_send(i).wait_send()

    loop(TILES, drain)


def module(scale, x, g, wv, wg, taps, gain, shift, wp):
    dma = pltpu.SemaphoreType.DMA
    vmem = pl.BlockSpec(memory_space=pltpu.VMEM)
    hbm = pl.BlockSpec(memory_space=pl.ANY)

    def half(rows, kind=F32):
        return pltpu.VMEM((2, rows, 128), kind)

    tile = pltpu.VMEM((TILES, T, 512), BF)
    return pl.pallas_call(
        functools.partial(whole, scale),
        out_shape=(
            jax.ShapeDtypeStruct((1024, 512), BF),
            jax.ShapeDtypeStruct((3, 32, 256), F32),
            jax.ShapeDtypeStruct((2, 40, 128), F32),
        ),
        in_specs=[hbm, hbm, hbm, hbm, vmem, vmem, vmem, hbm],
        out_specs=(vmem,) * 3,
        scratch_shapes=[
            pltpu.VMEM((1024, 2048), BF), pltpu.VMEM((1024, 2048), BF),
            pltpu.VMEM((2048, 256), BF), pltpu.VMEM((2048, 256), BF), pltpu.VMEM((256, 2048), BF),
            dma((8,)),
            half(1056), half(32), half(1024), half(1024), half(1024), half(1024), half(1056), half(32),
            pltpu.VMEM((1024, 512), BF), pltpu.VMEM((1024, 256), BF),
            pltpu.VMEM((2, TAPS, 8, 128), F32), pltpu.VMEM((2, 2, 8, 128), F32),
            pltpu.VMEM((T, 128), F32), pltpu.VMEM((T, 128), F32),
            pltpu.VMEM((TILES, T, 128), F32), pltpu.VMEM((TILES, T, 128), F32),
            pltpu.VMEM((T, 128), F32), pltpu.VMEM((T, 128), F32),
            pltpu.VMEM((TILES, 8, T), F32), pltpu.VMEM((TILES, 3, 8, T), F32),
            pltpu.VMEM((TILES, 8, T), F32), pltpu.VMEM((TILES, 3, 8, T), F32),
            pltpu.VMEM((3, TILES, T, 512), BF), pltpu.VMEM((TILES, T, 512), F32),
            tile, tile, tile,
            pltpu.VMEM((3, 32, 2, 32, 256), BF), pltpu.VMEM((3, 32, 32, 256), BF),
            pltpu.VMEM((3, 8, 4, 32, 256), BF), pltpu.VMEM((3, 3, 8, 32, 256), BF),
            pltpu.VMEM((3, 8, 32, 256), BF), pltpu.VMEM((3, 7, 32, 256), BF),
            pltpu.VMEM((6, 40, 128), F32), pltpu.VMEM((40, 128), F32),
            pltpu.VMEM((3, 40, 128), F32), pltpu.VMEM((7, 40, 128), F32),
            dma((2,)), dma((2,)),
            dma((TILES, 3)), dma((TILES, 3)), dma((TILES, 3)), dma((TILES, 3)),
            dma((TILES,)), dma((TILES,)), dma((TILES,)), dma((TILES,)), dma((TILES,)), dma((TILES,)),
            dma((3, 4)), dma((3, 4)), dma((3, 3, 2)), dma((3, 3, 2)), dma((3, 7)), dma((3, 7)),
            dma((12,)), dma((12,)),
        ],
        compiler_params=pltpu.CompilerParams(
            collective_id=0, has_side_effects=True, vmem_limit_bytes=62 * 1024 * 1024
        ),
        cost_estimate=pl.CostEstimate(
            flops=10_000_000_000, bytes_accessed=14_000_000, transcendentals=1_000_000
        ),
    )(x, g, wv, wg, taps, gain, shift, wp)


def placed(ig, w, sm, ig_out, v_out, g_out, p_out, t_out, gain_out, shift_out):
    ig_out[...] = ig[...]

    @pl.when(pl.program_id(0) == 0)
    def _():
        v_out[...] = w[1]
        g_out[...] = w[2]
        p_out[...] = w[0]
        for h in range(2):
            lanes = slice(h * 128, h * 128 + 128)
            t_out[:, lanes] = sm[h, 0:TAPS]
            gain_out[:, lanes] = sm[h, TAPS : TAPS + 1]
            shift_out[:, lanes] = sm[h, TAPS + 1 : TAPS + 2]


def fixed(*shape):
    return pl.BlockSpec(shape, lambda i: (0,) * len(shape))


def shards(block_input, out_grad, w_value, w_gate, conv_taps, norm_gain, norm_shift, w_proj):
    loss_scale = 1.0 / math.sqrt(block_input.shape[0] * lax.axis_size(SP))
    parts = module(
        loss_scale, block_input, out_grad, w_value, w_gate, conv_taps,
        norm_gain.reshape(1, -1), norm_shift.reshape(1, -1), w_proj,
    )
    shapes = [
        ((1024, 512), BF), ((32, 256), F32), ((32, 256), F32), ((32, 256), F32),
        ((TAPS, 256), F32), ((1, 256), F32), ((1, 256), F32),
    ]
    out = pl.pallas_call(
        placed,
        grid=(2,),
        in_specs=[pl.BlockSpec((512, 512), lambda i: (i, 0)), fixed(3, 32, 256), fixed(2, 40, 128)],
        out_specs=[pl.BlockSpec((512, 512), lambda i: (i, 0))]
        + [fixed(*shape) for shape, _ in shapes[1:]],
        out_shape=[jax.ShapeDtypeStruct(*shape) for shape in shapes],
        cost_estimate=pl.CostEstimate(flops=1_000_000, bytes_accessed=2_000_000, transcendentals=0),
    )(*parts)
    return (*out[:3], out[3].T, out[4], out[5].reshape(-1), out[6].reshape(-1))


def solution(mesh):
    return jax.shard_map(
        shards,
        mesh=mesh,
        in_specs=(
            P(SP, None),
            P(SP, None),
            P(None, "tp"),
            P(None, "tp"),
            P(None, "tp"),
            P("tp"),
            P("tp"),
            P("tp", None),
        ),
        out_specs=(
            P(SP, "tp"),
            P(SP, "tp"),
            P(SP, "tp"),
            P("tp", SP),
            P(None, "tp"),
            P("tp"),
            P("tp"),
        ),
        check_vma=False,
    )
```

```python
import functools
import math

import jax
import jax.numpy as jnp
from jax import lax
from jax.experimental import pallas as pl
from jax.experimental.pallas import tpu as pltpu
from jax.sharding import PartitionSpec as P

CH = 1024
SP = "sp"
MESH = pl.DeviceIdType.MESH
BF = jnp.bfloat16
F32 = jnp.float32
EPS = 0.05
TAPS = 31
T = 256
TILES = 4
R = 64
FAR_FIRST = (4, 3, 5, 2, 6, 1, 7)


def plain(left, right):
    return jnp.dot(left, right, preferred_element_type=F32)


def rows_product(left, right):
    return lax.dot_general(left, right, (((1,), (1,)), ((), ())), preferred_element_type=F32)


def cols_product(left, right):
    return lax.dot_general(left, right, (((0,), (0,)), ((), ())), preferred_element_type=F32)


def logistic(v):
    return 0.5 * jnp.tanh(0.5 * v) + 0.5


def loop(count, body):
    def step(i, carry):
        body(i)
        return carry

    lax.fori_loop(0, count, step, 0)


def whole(
    scale,
    x_h, g_h, wv_h, wg_h, taps, gain, shift, wp_h,
    ig_out, w_out, sm_out,
    x, g, wv, wg, wp, load,
    gi, gi_halo, vf, sg, filt, gm, gf, gf_halo, gb, mx, tg, gs,
    sum_a, sum_b, col_m, col_i, col_a, col_b, st1, got1, st2, got2,
    part, own, got_a, got_b, got_c,
    wbuf, got_w, s1, got_y, s2, got_z,
    smb, sm_c, sm_y, sm_z,
    hs, hr, t1s, t1r, t2s, t2r, as_, ar, bs, br, cs, cr,
    ws, wr, ys, yr, zs, zr, ms, mr,
):
    s = lax.axis_index(SP)
    t = lax.axis_index("tp")
    c, y, z = s % 2, (s // 2) % 4, s // 8
    right, left, far = (t + 1) % 4, (t + 3) % 4, (t + 2) % 4
    last_sp = 63

    def local(src, dst, k):
        return pltpu.make_async_copy(src, dst, load.at[k])

    def x_rows(i):
        rows = pl.ds(i * T, T)
        return local(x_h.at[rows], x.at[rows], i)

    loads = [local(wv_h, wv, 4), local(wg_h, wg, 5)]
    loads[0].start()
    x_rows(3).start()
    loads[1].start()
    for i in range(3):
        x_rows(i).start()
    late = [local(wp_h, wp, 6), local(g_h, g, 7)]
    for copy in late:
        copy.start()

    def at_y(k):
        return {SP: (z * 4 + (y + k) % 4) * 2 + c}

    def at_z(k):
        return {SP: (((z + k) % 8) * 4 + y) * 2 + c}

    def at_t(k):
        return {"tp": (t + k) % 4}

    partner = {SP: s + 1 - 2 * c}
    after = {SP: (s + 1) % 64}
    before = {SP: (s + 63) % 64}
    peers = [at_t(k) for k in (1, 2, 3)] + [partner, after, before]
    peers += [at_y(k) for k in (1, 2, 3)] + [at_z(k) for k in range(1, 8)]
    barrier = pltpu.get_barrier_semaphore()
    for peer in peers:
        pl.semaphore_signal(barrier, inc=1, device_id=peer, device_id_type=MESH)

    def remote(src, dst, ssem, rsem, device):
        return pltpu.make_async_remote_copy(
            src_ref=src, dst_ref=dst, send_sem=ssem, recv_sem=rsem,
            device_id=device, device_id_type=MESH,
        )

    tg[...] = jnp.zeros_like(tg)
    gs[...] = jnp.zeros_like(gs)
    st1[...] = jnp.zeros_like(st1)
    st2[...] = jnp.zeros_like(st2)

    def token_sums(tile):
        return jnp.sum(tile[...].T, axis=0, keepdims=True)

    def over_lanes(row):
        return jnp.broadcast_to(row, (128, T)).T


    halo_send = remote(gi.at[:, pl.ds(1024, 32)], gi_halo, hs.at[0], hr.at[0], after)
    grad_send = remote(gf.at[:, pl.ds(0, 32)], gf_halo, hs.at[1], hr.at[1], before)

    def st1_send(i, k):
        return remote(st1.at[i], got1.at[i, k - 1], t1s.at[i, k - 1], t1r.at[i, k - 1], at_t(k))

    def st2_send(i, k):
        return remote(st2.at[i], got2.at[i, k - 1], t2s.at[i, k - 1], t2r.at[i, k - 1], at_t(k))

    def project(i):
        rows = pl.ds(pl.multiple_of(i * T, T), T)
        x_rows(i).wait()
        value = plain(x[rows, :], wv[...]).astype(BF).astype(F32)
        gate = plain(x[rows, :], wg[...]).astype(BF).astype(F32)
        sig = logistic(gate)
        gated = (value * sig).astype(BF).astype(F32)
        at = pl.ds(pl.multiple_of(i * T + 32, 32), T)
        for h in range(2):
            lanes = slice(h * 128, h * 128 + 128)
            vf[h, rows, :] = value[:, lanes]
            sg[h, rows, :] = sig[:, lanes]
            gi[h, at, :] = gated[:, lanes]

    def filter_rows(i):
        def block(b):
            base = pl.multiple_of(i * T + b * 128, 128)
            rows = pl.ds(base, 128)
            tile = pl.ds(pl.multiple_of(b * 128, 128), 128)
            for h in range(2):
                acc = jnp.zeros((128, 128), F32)
                for k in range(TAPS):
                    tap = taps[k : k + 1, h * 128 : h * 128 + 128]
                    acc = acc + tap * gi[h, pl.ds(base + 32 - k, 128), :]
                filt[h, rows, :] = acc
                if h == 0:
                    sum_a[tile, :] = acc
                    sum_b[tile, :] = acc * acc
                else:
                    sum_a[tile, :] = sum_a[tile, :] + acc
                    sum_b[tile, :] = sum_b[tile, :] + acc * acc

        loop(T // 128, block)
        st1[i, 0:1] = token_sums(sum_a)
        st1[i, 1:2] = token_sums(sum_b)

    def filter_tell(i):
        for k in (2, 1, 3):
            st1_send(i, k).start()

    def filter_tile(i):
        filter_rows(i)
        filter_tell(i)

    def mixed(i):
        rows = pl.ds(pl.multiple_of(i * T, T), T)
        out = rows_product(g[rows, :], wp[...])
        for h in range(2):
            gm[h, rows, :] = out[:, h * 128 : h * 128 + 128]

    def activate(i):
        for k in (1, 2, 3):
            st1_send(i, k).wait_recv()
        sums = st1[i] + got1[i, 0] + got1[i, 1] + got1[i, 2]
        mean = sums[0:1] / CH
        var = sums[1:2] / CH - mean * mean
        col_m[i] = over_lanes(mean)
        col_i[i] = over_lanes(lax.rsqrt(var + EPS))

        def block(b):
            local_rows = pl.ds(pl.multiple_of(b * R, R), R)
            rows = pl.ds(pl.multiple_of(i * T + b * R, R), R)
            mean = col_m[i, local_rows, :]
            inv = col_i[i, local_rows, :]
            first, second = 0.0, 0.0
            for h in range(2):
                lanes = slice(h * 128, h * 128 + 128)
                normed = (filt[h, rows, :] - mean) * inv
                act = normed * gain[0:1, lanes] + shift[0:1, lanes]
                sig = logistic(act)
                mx[rows, lanes] = (act * sig).astype(BF)
                grad = gm[h, rows, :] * sig * (1.0 + act * (1.0 - sig))
                gs[0, h] = gs[0, h] + (grad * normed).reshape(R // 8, 8, 128).sum(axis=0)
                gs[1, h] = gs[1, h] + grad.reshape(R // 8, 8, 128).sum(axis=0)
                grad = grad * gain[0:1, lanes]
                filt[h, rows, :] = normed
                gm[h, rows, :] = grad
                first = first + grad
                second = second + grad * normed
            sum_a[local_rows, :] = first
            sum_b[local_rows, :] = second

        loop(T // R, block)
        st2[i, 0:1] = token_sums(sum_a)
        st2[i, 1:2] = token_sums(sum_b)
        for k in (2, 1, 3):
            st2_send(i, k).start()

    def pair_send(n, q):
        rows = pl.ds(q * 8, 8)
        return remote(
            wbuf.at[n, rows, 1 - c], got_w.at[n, rows], ws.at[n, q], wr.at[n, q], partner
        )

    def y_way(q):
        return jnp.where(q == 0, (y + 1) % 4, (y + 3) % 4), jnp.where(q == 0, (y + 3) % 4, (y + 1) % 4)

    def y_move(kind, n, q, which, line):
        rows = pl.ds(q * 4, 4)
        return remote(
            s1.at[n, rows, which], got_y.at[kind, n, rows], ys.at[kind, n, q], yr.at[kind, n, q],
            {SP: (z * 4 + line) * 2 + c},
        )

    def ya_send(n, q):
        return y_move(0, n, q, (y + 2) % 4, y_way(q)[0])

    def yb_send(n, q):
        return y_move(1, n, q, y_way(q)[1], y_way(q)[1])

    def yc_send(n, q):
        return y_move(2, n, q, y_way(q)[0], y_way(q)[0])

    def z_send(n, k):
        return remote(
            s2.at[n, (z + k) % 8], got_z.at[n, k - 1], zs.at[n, k - 1], zr.at[n, k - 1], at_z(k)
        )

    def proj_half(first):
        def tile(j):
            zb = first + j
            span = pl.ds(pl.multiple_of(zb * 512, 512), 512)
            out = cols_product(g[:, span], mx[...]).astype(BF)
            wbuf[0, pl.ds(zb * 8, 8)] = out.reshape(8, 2, 32, 256)
            pair_send(0, zb).start()

        loop(2, tile)

    def gate_chunks(first, count):
        def tile(j):
            zb = first + j
            span = pl.ds(pl.multiple_of(zb * 512, 512), 512)
            out = cols_product(x[:, span], gb[...]).astype(BF)
            for n in (0, 1):
                wbuf[n + 1, pl.ds(zb * 8, 8)] = out[:, n * 256 : n * 256 + 256].reshape(8, 2, 32, 256)
                pair_send(n + 1, zb).start()

        loop(count, tile)

    def pair_half(n, q):
        def tile(j):
            pair_send(n, q * 2 + j).wait_recv()
            for r in range(2):
                rows = pl.ds(q * 8 * 2 + j * 8 + r * 4, 4)
                s1[n, q * 4 + j * 2 + r] = wbuf[n, rows, c] + got_w[n, rows]

        loop(2, tile)
        ya_send(n, q).start()
        yb_send(n, q).start()

    def pair_sum(n):
        pair_half(n, 0)
        pair_half(n, 1)

    def y_pass(n):
        for q in (0, 1):
            ya_send(n, q).wait_recv()
            rows, line = pl.ds(q * 4, 4), y_way(q)[0]
            s1[n, rows, line] = s1[n, rows, line] + got_y[0, n, rows]
            yc_send(n, q).start()

    def y_sum(n):
        for q in (0, 1):
            yb_send(n, q).wait_recv()
            yc_send(n, q).wait_recv()
        total = s1[n, :, y].astype(F32) + got_y[1, n].astype(F32) + got_y[2, n].astype(F32)
        s2[n] = total.astype(BF)
        for k in FAR_FIRST:
            z_send(n, k).start()

    def z_sum(n):
        for k in range(1, 8):
            z_send(n, k).wait_recv()
        total = s2[n, z].astype(F32)
        for k in range(7):
            total = total + got_z[n, k].astype(F32)
        w_out[n] = total * scale

    def filtered_grad(i):
        for k in (1, 2, 3):
            st2_send(i, k).wait_recv()
        sums = (st2[i] + got2[i, 0] + got2[i, 1] + got2[i, 2]) / CH
        col_a[...] = over_lanes(sums[0:1])
        col_b[...] = over_lanes(sums[1:2])

        def block(b):
            local_rows = pl.ds(pl.multiple_of(b * R, R), R)
            rows = pl.ds(pl.multiple_of(i * T + b * R, R), R)
            inv = col_i[i, local_rows, :]
            m1 = col_a[local_rows, :]
            m2 = col_b[local_rows, :]
            for h in range(2):
                gf[h, rows, :] = inv * (gm[h, rows, :] - m1 - filt[h, rows, :] * m2)

        loop(T // R, block)

    def toward(i):
        first = i < TILES // 2
        return jnp.where(first, right, left), jnp.where(first, left, right)

    def a_send(i):
        return remote(part.at[0, i], got_a.at[i], as_.at[i], ar.at[i], {"tp": toward(i)[0]})

    def b_send(i):
        return remote(part.at[1, i], got_b.at[i], bs.at[i], br.at[i], {"tp": toward(i)[1]})

    def c_send(i):
        return remote(part.at[2, i], got_c.at[i], cs.at[i], cr.at[i], {"tp": toward(i)[0]})

    def partial(i, block):
        rows = pl.ds(pl.multiple_of(i * T, T), T)
        span = pl.ds(pl.multiple_of(block * 512, 512), 512)
        return rows_product(gb[rows, 0:256], wv[span, :]) + rows_product(
            gb[rows, 256:512], wg[span, :]
        )

    def back_tile(i):
        for h in range(2):
            lanes = slice(h * 128, h * 128 + 128)
            lanes_g = slice(256 + h * 128, 384 + h * 128)

            def block(b, h=h, lanes=lanes, lanes_g=lanes_g):
                base = pl.multiple_of(i * T + b * R, R)
                rows = pl.ds(base, R)
                gated = gi[h, pl.ds(pl.multiple_of(base + 32, 32), R), :]
                acc = jnp.zeros((R, 128), F32)
                for k in range(TAPS):
                    moved = gf[h, pl.ds(base + k, R), :]
                    acc = acc + taps[k : k + 1, lanes] * moved
                    tg[h, k] = tg[h, k] + (gated * moved).reshape(R // 8, 8, 128).sum(axis=0)
                sig = sg[h, rows, :]
                gv = acc * sig
                gb[rows, lanes] = gv.astype(BF)
                gb[rows, lanes_g] = (gv * vf[h, rows, :] * (1.0 - sig)).astype(BF)

            loop(T // R, block)

        part[0, i] = partial(i, far).astype(BF)
        a_send(i).start()
        part[1, i] = partial(i, toward(i)[1]).astype(BF)
        b_send(i).start()

    def near_tile(i):
        part[2, i] = partial(i, toward(i)[0]).astype(BF)
        own[i] = partial(i, t)

    def combine(i):
        a_send(i).wait_recv()
        part[2, i] = part[2, i] + got_a[i]
        c_send(i).start()

    def gather(i):
        b_send(i).wait_recv()
        own[i] = own[i] + got_b[i].astype(F32)

    def pair(first, body):
        loop(2, lambda j: body(first + j))

    for copy in loads:
        copy.wait()
    loop(TILES, lambda j: project((j + 3) % 4))
    filter_rows(1)
    pl.semaphore_wait(barrier, len(peers))
    halo_send.start()
    filter_tell(1)
    pair(2, filter_tile)
    for copy in late:
        copy.wait()
    pair(1, mixed)
    halo_send.wait_recv()
    gi[:, 0:32, :] = jnp.where(s == 0, 0.0, gi_halo[...])
    filter_tile(0)
    pair(1, activate)
    loop(2, lambda j: mixed((j + 3) % 4))
    loop(2, lambda j: activate((j + 3) % 4))
    proj_half(0)
    pair(1, filtered_grad)

    def middle(j):
        @pl.when(j == 1)
        def _():
            proj_half(2)
            filtered_grad(3)
            filtered_grad(0)
            grad_send.start()

        @pl.when(j == 3)
        def _():
            pair_sum(0)
            grad_send.wait_recv()
            gf[:, 1024:1056, :] = jnp.where(s == last_sp, 0.0, gf_halo[...])

        back_tile(jnp.where(j == 3, 3, (j + 1) % 3))

    loop(TILES, middle)

    for h in range(2):
        smb[h, 0:TAPS] = jnp.sum(tg[h], axis=1)
        smb[h, 31:32] = jnp.sum(gs[0, h], axis=0, keepdims=True)
        smb[h, 32:33] = jnp.sum(gs[1, h], axis=0, keepdims=True)
        smb[h, 33:40] = jnp.zeros((7, 128), F32)
    sm_pair = remote(smb.at[1 - c], sm_c, ms.at[0], mr.at[0], partner)
    sm_pair.start()
    y_pass(0)
    gate_chunks(0, 3)
    loop(2, lambda j: pair_half(j + 1, 0))
    gate_chunks(3, 1)
    loop(TILES, near_tile)
    sm_pair.wait_recv()
    smb[2] = smb[c] + sm_c[...]
    sm_ys = [remote(smb.at[2], sm_y.at[k - 1], ms.at[k], mr.at[k], at_y(k)) for k in (2, 1, 3)]
    for copy in sm_ys:
        copy.start()
    loop(2, lambda j: pair_half(j + 1, 1))
    y_sum(0)
    combine(1)
    for copy in sm_ys:
        copy.wait_recv()
    smb[3] = smb[2] + sm_y[0] + sm_y[1] + sm_y[2]
    sm_zs = [
        remote(smb.at[3], sm_z.at[k - 1], ms.at[3 + k], mr.at[3 + k], at_z(k)) for k in FAR_FIRST
    ]
    for copy in sm_zs:
        copy.start()
    y_pass(1)
    combine(2)
    y_pass(2)
    combine(0)
    y_sum(1)
    y_sum(2)
    combine(3)
    for copy in sm_zs:
        copy.wait_recv()
    total = smb[3]
    for k in range(7):
        total = total + sm_z[k]
    smb[4] = total * scale
    sm_swap = remote(smb.at[4], smb.at[5], ms.at[11], mr.at[11], partner)
    sm_swap.start()
    loop(TILES, gather)
    z_sum(0)
    sm_swap.wait_recv()
    sm_out[c] = smb[4]
    sm_out[1 - c] = smb[5]
    loop(2, lambda j: z_sum(j + 1))

    def finish(i):
        c_send(i).wait_recv()
        rows = pl.ds(i * T, T)
        ig_out[rows, :] = (own[i] + got_c[i].astype(F32)).astype(BF)

    for i in (1, 2, 0, 3):
        finish(i)

    halo_send.wait_send()
    grad_send.wait_send()
    for copy in [sm_pair, sm_swap, *sm_ys, *sm_zs]:
        copy.wait_send()
    for n in range(3):
        for q in range(4):
            pair_send(n, q).wait_send()
        for q in (0, 1):
            ya_send(n, q).wait_send()
            yb_send(n, q).wait_send()
            yc_send(n, q).wait_send()
        for k in range(1, 8):
            z_send(n, k).wait_send()

    def drain(i):
        for k in (1, 2, 3):
            st1_send(i, k).wait_send()
            st2_send(i, k).wait_send()
        a_send(i).wait_send()
        b_send(i).wait_send()
        c_send(i).wait_send()

    loop(TILES, drain)


def module(scale, x, g, wv, wg, taps, gain, shift, wp):
    dma = pltpu.SemaphoreType.DMA
    vmem = pl.BlockSpec(memory_space=pltpu.VMEM)
    hbm = pl.BlockSpec(memory_space=pl.ANY)

    def half(rows, kind=F32):
        return pltpu.VMEM((2, rows, 128), kind)

    tile = pltpu.VMEM((TILES, T, 512), BF)
    return pl.pallas_call(
        functools.partial(whole, scale),
        out_shape=(
            jax.ShapeDtypeStruct((1024, 512), BF),
            jax.ShapeDtypeStruct((3, 32, 256), F32),
            jax.ShapeDtypeStruct((2, 40, 128), F32),
        ),
        in_specs=[hbm, hbm, hbm, hbm, vmem, vmem, vmem, hbm],
        out_specs=(vmem,) * 3,
        scratch_shapes=[
            pltpu.VMEM((1024, 2048), BF), pltpu.VMEM((1024, 2048), BF),
            pltpu.VMEM((2048, 256), BF), pltpu.VMEM((2048, 256), BF), pltpu.VMEM((256, 2048), BF),
            dma((8,)),
            half(1056), half(32), half(1024), half(1024), half(1024), half(1024), half(1056), half(32),
            pltpu.VMEM((1024, 512), BF), pltpu.VMEM((1024, 256), BF),
            pltpu.VMEM((2, TAPS, 8, 128), F32), pltpu.VMEM((2, 2, 8, 128), F32),
            pltpu.VMEM((T, 128), F32), pltpu.VMEM((T, 128), F32),
            pltpu.VMEM((TILES, T, 128), F32), pltpu.VMEM((TILES, T, 128), F32),
            pltpu.VMEM((T, 128), F32), pltpu.VMEM((T, 128), F32),
            pltpu.VMEM((TILES, 8, T), F32), pltpu.VMEM((TILES, 3, 8, T), F32),
            pltpu.VMEM((TILES, 8, T), F32), pltpu.VMEM((TILES, 3, 8, T), F32),
            pltpu.VMEM((3, TILES, T, 512), BF), pltpu.VMEM((TILES, T, 512), F32),
            tile, tile, tile,
            pltpu.VMEM((3, 32, 2, 32, 256), BF), pltpu.VMEM((3, 32, 32, 256), BF),
            pltpu.VMEM((3, 8, 4, 32, 256), BF), pltpu.VMEM((3, 3, 8, 32, 256), BF),
            pltpu.VMEM((3, 8, 32, 256), BF), pltpu.VMEM((3, 7, 32, 256), BF),
            pltpu.VMEM((6, 40, 128), F32), pltpu.VMEM((40, 128), F32),
            pltpu.VMEM((3, 40, 128), F32), pltpu.VMEM((7, 40, 128), F32),
            dma((2,)), dma((2,)),
            dma((TILES, 3)), dma((TILES, 3)), dma((TILES, 3)), dma((TILES, 3)),
            dma((TILES,)), dma((TILES,)), dma((TILES,)), dma((TILES,)), dma((TILES,)), dma((TILES,)),
            dma((3, 4)), dma((3, 4)), dma((3, 3, 2)), dma((3, 3, 2)), dma((3, 7)), dma((3, 7)),
            dma((12,)), dma((12,)),
        ],
        compiler_params=pltpu.CompilerParams(
            collective_id=0, has_side_effects=True, vmem_limit_bytes=62 * 1024 * 1024
        ),
        cost_estimate=pl.CostEstimate(
            flops=10_000_000_000, bytes_accessed=14_000_000, transcendentals=1_000_000
        ),
    )(x, g, wv, wg, taps, gain, shift, wp)


def placed(ig, w, sm, ig_out, v_out, g_out, p_out, t_out, gain_out, shift_out):
    ig_out[...] = ig[...]

    @pl.when(pl.program_id(0) == 0)
    def _():
        v_out[...] = w[1]
        g_out[...] = w[2]
        p_out[...] = w[0]
        for h in range(2):
            lanes = slice(h * 128, h * 128 + 128)
            t_out[:, lanes] = sm[h, 0:TAPS]
            gain_out[:, lanes] = sm[h, TAPS : TAPS + 1]
            shift_out[:, lanes] = sm[h, TAPS + 1 : TAPS + 2]


def fixed(*shape):
    return pl.BlockSpec(shape, lambda i: (0,) * len(shape))


def shards(block_input, out_grad, w_value, w_gate, conv_taps, norm_gain, norm_shift, w_proj):
    loss_scale = 1.0 / math.sqrt(block_input.shape[0] * lax.axis_size(SP))
    parts = module(
        loss_scale, block_input, out_grad, w_value, w_gate, conv_taps,
        norm_gain.reshape(1, -1), norm_shift.reshape(1, -1), w_proj,
    )
    shapes = [
        ((1024, 512), BF), ((32, 256), F32), ((32, 256), F32), ((32, 256), F32),
        ((TAPS, 256), F32), ((1, 256), F32), ((1, 256), F32),
    ]
    out = pl.pallas_call(
        placed,
        grid=(2,),
        in_specs=[pl.BlockSpec((512, 512), lambda i: (i, 0)), fixed(3, 32, 256), fixed(2, 40, 128)],
        out_specs=[pl.BlockSpec((512, 512), lambda i: (i, 0))]
        + [fixed(*shape) for shape, _ in shapes[1:]],
        out_shape=[jax.ShapeDtypeStruct(*shape) for shape in shapes],
        cost_estimate=pl.CostEstimate(flops=1_000_000, bytes_accessed=2_000_000, transcendentals=0),
    )(*parts)
    return (*out[:3], out[3].T, out[4], out[5].reshape(-1), out[6].reshape(-1))


def solution(mesh):
    return jax.shard_map(
        shards,
        mesh=mesh,
        in_specs=(
            P(SP, None),
            P(SP, None),
            P(None, "tp"),
            P(None, "tp"),
            P(None, "tp"),
            P("tp"),
            P("tp"),
            P("tp", None),
        ),
        out_specs=(
            P(SP, "tp"),
            P(SP, "tp"),
            P(SP, "tp"),
            P("tp", SP),
            P(None, "tp"),
            P("tp"),
            P("tp"),
        ),
        check_vma=False,
    )
```
